128 devices in a mesh: sp: 16 (over z, x), tp: 8 (over y, core).
Axes of the slice: x: 4, y: 4, z: 4, core: 2. Of those that a mesh axis runs over, the one named last changes fastest.
Arguments:
- tokens: bfloat16 [16384, 2048], P(('sp', 'tp')), may hold values from -6 to 6
- elapsed: float32 [16384], P(('sp', 'tp')), may hold values from 0 to 3, as said below
- norm_gain: float32 [2048], replicated, may hold values from 0.1 to 1.9
- in_weight: bfloat16 [2048, 1024], replicated, may hold values from -0.125 to 0.125
- state_input: bfloat16 [2, 2, 64, 64, 16], replicated, may hold values from -1.5 to 1.5
- state_output: float32 [2, 2, 64, 16, 64], replicated, may hold values from -0.375 to 0.375
- forget_rate: float32 [2, 64, 64], replicated, may hold values from 0 to 1, as said below
- decay_angle: float32 [2, 64, 64], replicated, may hold values from -3.140625 to 3.140625
- skip_gain: float32 [1024], replicated, may hold values from -4 to 4
- glu_weight: bfloat16 [1024, 1024], replicated, may hold values from -0.1875 to 0.1875
- glu_bias: float32 [1024], replicated, may hold values from -4 to 4
- out_weight: bfloat16 [1024, 2048], replicated, may hold values from -0.1875 to 0.1875
- out_gain: float32 [2048], replicated, may hold values from 0.1 to 1.9
Outputs:
- mixed: bfloat16 [16384, 2048], P(('sp', 'tp'))
The draws below stay inside these ranges and needn't reach their ends.
Inputs may be any that keep to these rules, and one draw needn't show every extreme that they name: `elapsed`: positive time steps. `forget_rate`: positive rates.
All inputs are finite; a program needn't handle non-finite values.
Results may differ from the reference program's by a relative error of at most 0.0067.
Values sent between devices are 32-bit elements; how exact they have to be, the bound alone decides.
A program may use at most 128 MiB of HBM per device.

```python
import math
import jax
import jax.numpy as jnp
from jax import lax

D = 2048
GROUPS = 64
WIDTH = 16
STATE = 64
CHANNELS = 1024
TOK_DEV = 128
SEQ = 16384


def draw_elapsed(key, part):
    first_key, second_key = jax.random.split(key)
    factor = jnp.exp(jax.random.uniform(first_key, (64,), jnp.float32, math.log(0.5), math.log(2.0)))
    jitter = jax.random.uniform(second_key, (SEQ,), jnp.float32, 0.7, 1.4)
    return jnp.repeat(factor, SEQ // 64, total_repeat_length=SEQ) * jitter


def draw_forget_rate(key, part):
    pick_key, quick_key, slow_key = jax.random.split(key, 3)
    share = 0.5
    quick_groups = jax.random.bernoulli(pick_key, share, (2, GROUPS, 1))
    quick = jnp.exp(jax.random.uniform(quick_key, (2, GROUPS, STATE), jnp.float32, math.log(1.0 / 100.0), math.log(1.0 / 30.0)))
    slow = jnp.exp(jax.random.uniform(slow_key, (2, GROUPS, STATE), jnp.float32, math.log(0.05 / SEQ), math.log(2.0 / SEQ)))
    return jnp.where(quick_groups, quick, slow)


def steps_of(stream_key, shape, cuts, low, top_value):
    def one(position, shards_of):
        steps = jax.random.uniform(jax.random.fold_in(jax.random.fold_in(stream_key, 6), position), (shards_of,), jnp.float32, low / len(cuts), top_value / len(cuts))
        return jnp.repeat(jnp.exp(steps), shape[position] // shards_of).reshape((-1,) + (1,) * (len(shape) - position - 1))

    gain = one(*cuts[0])
    for cut in cuts[1:]:
        gain = gain * one(*cut)
    return gain


def centred(key, extent, deviation, reach, pieces=(), dtype=jnp.bfloat16):
    loudness = steps_of(key, extent, pieces, -0.22, 0.18) if pieces else 1.0
    values = jax.random.normal(key, extent, jnp.float32) * deviation * loudness
    return jnp.minimum(jnp.maximum(values, -reach), reach).astype(dtype)


def setup_inputs(seed: int = 0) -> dict:
    splits = jax.random.split(jax.random.key(seed), 14)
    tokens = centred(splits[0], (SEQ, D), 1.0, 6.0, ((0, 128),))
    elapsed = draw_elapsed(jax.random.fold_in(splits[13], 71), 0)
    norm_gain = jnp.clip(1.0 + 0.18 * jax.random.normal(splits[2], (D,), jnp.float32), 0.1, 1.9)
    in_weight = centred(splits[3], (D, CHANNELS), D ** -0.5, 0.125)
    state_input = centred(splits[4], (2, 2, GROUPS, STATE, WIDTH), WIDTH ** -0.5, 1.5)
    state_output = centred(splits[5], (2, 2, GROUPS, WIDTH, STATE), (4 * STATE) ** -0.5, 0.375, (), jnp.float32)
    forget_rate = draw_forget_rate(jax.random.fold_in(splits[13], 71), 0)
    decay_angle = jnp.clip(jax.random.uniform(splits[7], (2, GROUPS, STATE), jnp.float32, -3.140625, 3.140625), -3.140625, 3.140625)
    skip_gain = centred(splits[8], (CHANNELS,), 1.0, 4.0, (), jnp.float32)
    glu_weight = centred(splits[9], (CHANNELS, CHANNELS), CHANNELS ** -0.5, 0.1875)
    glu_bias = centred(splits[10], (CHANNELS,), 1.0, 4.0, (), jnp.float32)
    out_weight = centred(splits[11], (CHANNELS, D), CHANNELS ** -0.5, 0.1875)
    out_gain = jnp.clip(1.0 + 0.18 * jax.random.normal(splits[12], (D,), jnp.float32), 0.1, 1.9)
    return dict(tokens=tokens, elapsed=elapsed, norm_gain=norm_gain, in_weight=in_weight, state_input=state_input, state_output=state_output, forget_rate=forget_rate, decay_angle=decay_angle, skip_gain=skip_gain, glu_weight=glu_weight, glu_bias=glu_bias, out_weight=out_weight, out_gain=out_gain)


epsilon = 1e-06

def rms_scale(activations, gain_row):
    values = activations.astype(jnp.float32)
    return values * lax.rsqrt(lax.optimization_barrier(jnp.mean(values * values, axis=-1, keepdims=True)) + epsilon) * gain_row

def read_out(state_re, state_im, readout):
    count = state_re.shape[0]
    groups, group_width, states = (readout.shape[1], readout.shape[2], readout.shape[3])
    real_part = jnp.einsum('tgp,ghp->tgh', state_re.reshape(count, groups, states), readout[0], precision=lax.Precision.HIGHEST)
    imag_part = jnp.einsum('tgp,ghp->tgh', state_im.reshape(count, groups, states), readout[1], precision=lax.Precision.HIGHEST)
    return (real_part - imag_part).reshape(count, groups * group_width)

def direction_pass(driven, elapsed, inputs, readout, rate, angle, backward):
    cell_count = rate.shape[0]

    def block_step(state, piece):
        block_rows, block_steps = piece
        grouped = block_rows.astype(jnp.float32).reshape(TOK_DEV, GROUPS, WIDTH)
        proj_re = jnp.einsum('tgh,gph->tgp', grouped, inputs[0]).reshape(TOK_DEV, cell_count)
        proj_im = jnp.einsum('tgh,gph->tgp', grouped, inputs[1]).reshape(TOK_DEV, cell_count)
        steps_col = block_steps[:, None]
        damping = jnp.sqrt(-jnp.expm1(-2.0 * rate * steps_col))
        fade = jnp.exp(-rate * steps_col)
        angles = angle * steps_col
        decay_re = fade * jnp.cos(angles)
        decay_im = fade * jnp.sin(angles)

        def token_step(carry, item):
            old_re, old_im = carry
            step_re, step_im, push_re, push_im = item
            new_re = step_re * old_re - step_im * old_im + push_re
            new_im = step_re * old_im + step_im * old_re + push_im
            return ((new_re, new_im), (new_re, new_im))
        state, outputs = lax.scan(token_step, state, (decay_re, decay_im, proj_re * damping, proj_im * damping), reverse=backward)
        return (state, read_out(outputs[0], outputs[1], readout))
    start = (jnp.zeros((cell_count,), jnp.float32), jnp.zeros((cell_count,), jnp.float32))
    _, result = lax.scan(block_step, start, (driven, elapsed), reverse=backward)
    return result

def reference(tokens, elapsed, norm_gain, in_weight, state_input, state_output, forget_rate, decay_angle, skip_gain, glu_weight, glu_bias, out_weight, out_gain):
    normed = rms_scale(tokens, norm_gain).astype(jnp.bfloat16)
    driven = jnp.dot(normed, in_weight, preferred_element_type=jnp.float32).astype(jnp.bfloat16)
    response = skip_gain * driven.astype(jnp.float32)
    block_count = SEQ // TOK_DEV
    for direction in range(2):
        part_out = direction_pass(driven.reshape(block_count, TOK_DEV, CHANNELS), elapsed.reshape(block_count, TOK_DEV), state_input[direction].astype(jnp.float32), state_output[direction], forget_rate[direction].reshape(-1), decay_angle[direction].reshape(-1), direction == 1)
        response = response + part_out.reshape(SEQ, CHANNELS)
    active = jax.nn.gelu(response)
    gate_pre = jnp.dot(active.astype(jnp.bfloat16), glu_weight, preferred_element_type=jnp.float32) + glu_bias
    gated = (active * jax.nn.sigmoid(gate_pre)).astype(jnp.bfloat16)
    projected = jnp.dot(gated, out_weight, preferred_element_type=jnp.float32)
    return rms_scale(projected, out_gain).astype(jnp.bfloat16)
```

```python
import functools
import math

import jax
import jax.numpy as jnp
from jax import lax
from jax.experimental import pallas as pl
from jax.experimental.pallas import tpu as pltpu
from jax.sharding import PartitionSpec as P

F32 = jnp.float32
BF16 = jnp.bfloat16
MESH = pl.DeviceIdType.MESH

ROWS = 128
TILES = 32
SUBS = 8
STEPS = 16
NEAR = 4
EPS = 1e-06
LOG2E = 1.4426950408889634
SIN_C = (4.442883014678955, -7.308241367340088, 3.6062889099121094, -0.845763623714447, 0.10920575261116028)
COS_C = (1.4142135381698608, -6.9788641929626465, 5.73988151550293, -1.8882750272750854, 0.3322518765926361, -0.034502167254686356)
INV_TURN = 1.0 / (2.0 * math.pi)
TURN_HI = math.floor(INV_TURN * 4096.0) / 4096.0
TURN_LO = INV_TURN - TURN_HI


def horner(x, coefficients):
    total = coefficients[-1]
    for c in coefficients[-2::-1]:
        total = total * x + c
    return total


def half_turn_parts(turns):
    part = turns - lax.round(turns, lax.RoundingMethod.TO_NEAREST_EVEN)
    square = part * part
    return part * horner(square, SIN_C), horner(square, COS_C)


def decay_parts(size, turns):
    sine, cosine = half_turn_parts(turns)
    lean = size * sine
    return size - lean * sine, lean * cosine


def times(a_re, a_im, b_re, b_im):
    return a_re * b_re - a_im * b_im, a_re * b_im + a_im * b_re


def kernel(
    tokens_h, elapsed_h, ngain_h, inw_h, sin_h, sout_h, rate_h, angle_h, skip_h, glu_h, gbias_h, outw_h, ogain_h,
    out_ref,
    tokens_v, elapsed_v, ngain_v, inw_v, sin_v, sout_v, rate_v, angle_v, skip_v, glu_v, gbias_v, outw_v, ogain_v,
    normed, acc, drv, resp, bst, cst, proj, dec, tabs, dts, spans, loc, ssum, lead, fade, ent,
    t_own, t_par, t_y, t_x, t_z, s_par, s_y, s_x, s_z, s_fin, s_in,
    dma_sem, t_send, t_recv, d_send, d_recv,
):
    sp = lax.axis_index("sp")
    tp = lax.axis_index("tp")
    zi, xi = sp // NEAR, sp % NEAR
    yi, core = tp // 2, tp % 2
    way = 1 - core

    def partner():
        return {"sp": sp, "tp": yi * 2 + (1 - core)}

    def along(axis, q):
        if axis == "y":
            return {"sp": sp, "tp": q * 2 + core}
        if axis == "x":
            return {"sp": zi * NEAR + q, "tp": tp}
        return {"sp": q * NEAR + xi, "tp": tp}

    own = {"y": yi, "x": xi, "z": zi}

    pairs = [
        (elapsed_h, elapsed_v), (tokens_h, tokens_v), (ngain_h, ngain_v), (rate_h, rate_v), (angle_h, angle_v),
        (sin_h, sin_v), (sout_h, sout_v), (skip_h, skip_v), (gbias_h, gbias_v), (glu_h, glu_v),
        (ogain_h, ogain_v), (outw_h, outw_v),
    ]
    copies = [pltpu.make_async_copy(a, b, dma_sem.at[k]) for k, (a, b) in enumerate(pairs)]
    c_el, c_tok, c_ng, c_rate, c_ang, c_sin, c_sout, c_skip, c_gb, c_glu, c_og, c_ow = copies
    in_copies = [
        pltpu.make_async_copy(inw_h.at[pl.ds(k * 512, 512), :], inw_v.at[pl.ds(k * 512, 512), :], dma_sem.at[12 + k])
        for k in range(4)
    ]
    for c in (c_el, c_tok, c_ng, c_rate, c_ang):
        c.start()
    for c in in_copies:
        c.start()
    for c in (c_sin, c_sout, c_skip, c_gb, c_glu, c_og, c_ow):
        c.start()

    barrier = pltpu.get_barrier_semaphore()
    pl.semaphore_signal(barrier, inc=1, device_id=partner(), device_id_type=MESH)
    for axis in "yxz":
        for k in range(1, NEAR):
            peer = along(axis, lax.rem(own[axis] + k, NEAR))
            pl.semaphore_signal(barrier, inc=1, device_id=peer, device_id_type=MESH)

    c_el.wait()
    steps = elapsed_v[...]
    whole = jnp.floor(steps)
    rest = steps - whole
    lane8 = lax.broadcasted_iota(jnp.int32, (SUBS, 128), 1)
    sub8 = lax.broadcasted_iota(jnp.int32, (SUBS, 128), 0)

    def picked(mask, row):
        total = jnp.sum(jnp.where(mask, jnp.broadcast_to(row, (SUBS, 128)), 0.0), axis=1, keepdims=True)
        return jnp.broadcast_to(total, (SUBS, 128))

    t_own[...] = jnp.where(sub8 == 0, picked(lane8 >= 0, whole), picked(lane8 >= 0, rest))
    for j in range(STEPS):
        dts[j] = picked(lane8 == sub8 * STEPS + j, steps)
    stretch = lane8 // STEPS
    for k, mask in enumerate((stretch == sub8, stretch > sub8, stretch < sub8)):
        spans[2 * k] = picked(mask, whole)
        spans[2 * k + 1] = picked(mask, rest)

    pl.semaphore_wait(barrier, 1 + 3 * (NEAR - 1))

    def t_core():
        return pltpu.make_async_remote_copy(
            src_ref=t_own, dst_ref=t_par, send_sem=t_send.at[0], recv_sem=t_recv.at[0],
            device_id=partner(), device_id_type=MESH,
        )

    def t_stage(axis, buf, base):
        me = own[axis]
        made = []
        for k in range(1, NEAR):
            q = lax.rem(me + k, NEAR)
            made.append(pltpu.make_async_remote_copy(
                src_ref=buf.at[me], dst_ref=buf.at[me], send_sem=t_send.at[base + k],
                recv_sem=t_recv.at[base + me], device_id=along(axis, q), device_id_type=MESH,
            ))
        return made

    def t_arrived(axis, buf, base):
        me = own[axis]
        for k in range(1, NEAR):
            q = lax.rem(me + k, NEAR)
            pltpu.make_async_remote_copy(
                src_ref=buf.at[q], dst_ref=buf.at[q], send_sem=t_send.at[base + k],
                recv_sem=t_recv.at[base + q], device_id=along(axis, q), device_id_type=MESH,
            ).wait_recv()

    t_core().start()

    c_rate.wait()
    c_ang.wait()
    for d in range(2):
        rate = jnp.concatenate([rate_v[d, 0:TILES, :], rate_v[d, TILES:, :]], axis=1)
        angle = jnp.concatenate([angle_v[d, 0:TILES, :], angle_v[d, TILES:, :]], axis=1)
        tabs[d, 0] = rate * (-LOG2E)
        tabs[d, 1] = rate * 2.0
        big = lax.round(angle * 1024.0, lax.RoundingMethod.TO_NEAREST_EVEN) * (1.0 / 1024.0)
        small = angle - big
        first = big * TURN_HI
        second = big * TURN_LO + (small * TURN_HI + small * TURN_LO)
        high = lax.round(first * 256.0, lax.RoundingMethod.TO_NEAREST_EVEN) * (1.0 / 256.0)
        low = (first - high) + second
        tabs[d, 2] = high
        tabs[d, 3] = low
        tabs[d, 4] = high + low

    def stretch_decay(rate2, high, low, both, t_whole, t_rest):
        size = jnp.exp2(rate2 * (t_whole + t_rest))
        turns = high * t_whole
        turns = turns - lax.round(turns, lax.RoundingMethod.TO_NEAREST_EVEN)
        return decay_parts(size, turns + low * t_whole + both * t_rest)

    def table_decay(d, t_tile):
        t_whole = jnp.broadcast_to(t_tile[0:1, :], (TILES, 128))
        t_rest = jnp.broadcast_to(t_tile[1:2, :], (TILES, 128))
        return stretch_decay(tabs[d, 0], tabs[d, 2], tabs[d, 3], tabs[d, 4], t_whole, t_rest)

    c_tok.wait()
    c_ng.wait()
    for r in range(4):
        x = tokens_v[pl.ds(r * 32, 32), :].astype(F32)
        scale = lax.rsqrt(jnp.mean(x * x, axis=-1, keepdims=True) + EPS)
        normed[pl.ds(r * 32, 32), :] = (x * scale * ngain_v[...]).astype(BF16)

    t_core().wait_recv()
    t_y[yi] = t_own[...] + t_par[...]
    for c in t_stage("y", t_y, 1):
        c.start()

    for k in range(2):
        in_copies[k].wait()
        part = jnp.dot(normed[:, k * 512:(k + 1) * 512], inw_v[k * 512:(k + 1) * 512, :], preferred_element_type=F32)
        acc[...] = part if k == 0 else acc[...] + part
    t_arrived("y", t_y, 1)
    t_x[xi] = t_y[0] + t_y[1] + t_y[2] + t_y[3]
    for c in t_stage("x", t_x, 5):
        c.start()
    for k in range(2, 4):
        in_copies[k].wait()
        acc[...] += jnp.dot(normed[:, k * 512:(k + 1) * 512], inw_v[k * 512:(k + 1) * 512, :], preferred_element_type=F32)

    row_i = lax.broadcasted_iota(jnp.int32, (ROWS, ROWS), 0)
    col_i = lax.broadcasted_iota(jnp.int32, (ROWS, ROWS), 1)
    order = jnp.where(col_i == (row_i % SUBS) * STEPS + row_i // SUBS, 1.0, 0.0).astype(BF16)
    back = jnp.where(row_i == (col_i % SUBS) * STEPS + col_i // SUBS, 1.0, 0.0).astype(BF16)

    driven = jnp.dot(order, acc[...].astype(BF16), preferred_element_type=F32)
    c_skip.wait()
    for m in range(4):
        low_d, high_d = driven[:, m * 128:(m + 1) * 128], driven[:, 512 + m * 128:512 + (m + 1) * 128]
        resp[m, :, 0:128] = low_d * skip_v[:, m * 128:(m + 1) * 128]
        resp[m, :, 128:256] = high_d * skip_v[:, 512 + m * 128:512 + (m + 1) * 128]
        drv[m, :, 0:128] = low_d.astype(BF16)
        drv[m, :, 128:256] = high_d.astype(BF16)

    t_arrived("x", t_x, 5)
    t_z[zi] = t_x[0] + t_x[1] + t_x[2] + t_x[3]
    for c in t_stage("z", t_z, 9):
        c.start()

    c_sin.wait()
    nothing = jnp.zeros((128, 64), BF16)
    for m in range(4):
        for d in range(2):
            for part in range(2):
                at = (d * 2 + part) * 128
                lower = sin_v[d, part, m * 8:(m + 1) * 8].reshape(128, 64)
                upper = sin_v[d, part, TILES + m * 8:TILES + (m + 1) * 8].reshape(128, 64)
                bst[m, 0:128, at:at + 128] = jnp.concatenate([lower, nothing], axis=1)
                bst[m, 128:256, at:at + 128] = jnp.concatenate([nothing, upper], axis=1)

    group_lane = (lax.broadcasted_iota(jnp.int32, (ROWS, 256), 1) // 16) % 8

    def project(tile, carry):
        m, i = tile // 8, tile % 8
        lhs = jnp.where(group_lane == i, drv[m].astype(F32), 0.0).astype(BF16)
        proj[tile] = jnp.dot(lhs, bst[m], preferred_element_type=F32)
        return carry

    lax.fori_loop(0, TILES, project, 0)

    def first_pass(tile, carry):
        rows = []
        for d in range(2):
            line = [jnp.broadcast_to(tabs[d, k, pl.ds(tile, 1), :], (SUBS, 128)) for k in range(5)]
            rate2, double, high, low, both = line
            s_re = s_im = None
            base = d * 256
            for j in range(STEPS) if d == 0 else range(STEPS - 1, -1, -1):
                dt = dts[j]
                at = pl.ds(j * SUBS, SUBS)
                size = jnp.exp2(rate2 * dt)
                a_re, a_im = decay_parts(size, both * dt)
                y = double * dt
                near = y * horner(y, (1.0, -0.5, 1.0 / 6.0, -1.0 / 24.0))
                gap = jnp.where(y < 0.03, near, 1.0 - size * size)
                damp = gap * lax.rsqrt(jnp.maximum(gap, 1e-37))
                p_re = proj[tile, at, base:base + 128] * damp
                p_im = proj[tile, at, base + 128:base + 256] * damp
                proj[tile, at, base:base + 128] = p_re
                proj[tile, at, base + 128:base + 256] = p_im
                dec[tile, at, base:base + 128] = a_re
                dec[tile, at, base + 128:base + 256] = a_im
                if s_re is None:
                    s_re, s_im = p_re, p_im
                else:
                    n_re, n_im = times(a_re, a_im, s_re, s_im)
                    s_re, s_im = n_re + p_re, n_im + p_im
            loc[tile, d, 0] = s_re
            loc[tile, d, 1] = s_im
            k = 2 if d == 0 else 4
            w_re, w_im = stretch_decay(rate2, high, low, both, spans[k], spans[k + 1])
            m_re, m_im = times(w_re, w_im, s_re, s_im)
            ssum[d, 0, pl.ds(tile, 1), :] = jnp.sum(m_re, axis=0, keepdims=True)
            ssum[d, 1, pl.ds(tile, 1), :] = jnp.sum(m_im, axis=0, keepdims=True)
        return carry

    lax.fori_loop(0, TILES, first_pass, 0)

    def d_core():
        return pltpu.make_async_remote_copy(
            src_ref=ssum.at[core], dst_ref=s_par, send_sem=d_send.at[0], recv_sem=d_recv.at[0],
            device_id=partner(), device_id_type=MESH,
        )

    def d_stage(axis, buf, base):
        me = own[axis]
        return [
            pltpu.make_async_remote_copy(
                src_ref=buf.at[me], dst_ref=buf.at[me], send_sem=d_send.at[base + k], recv_sem=d_recv.at[base + me],
                device_id=along(axis, lax.rem(me + k, NEAR)), device_id_type=MESH,
            )
            for k in range(1, NEAR)
        ]

    def d_arrived(axis, buf, base):
        me = own[axis]
        for k in range(1, NEAR):
            q = lax.rem(me + k, NEAR)
            pltpu.make_async_remote_copy(
                src_ref=buf.at[q], dst_ref=buf.at[q], send_sem=d_send.at[base + k], recv_sem=d_recv.at[base + q],
                device_id=along(axis, q), device_id_type=MESH,
            ).wait_recv()

    def walk(axis, sbuf, tbuf):
        me = own[axis]
        run = (jnp.zeros((TILES, 128), F32), jnp.zeros((TILES, 128), F32))
        run_d = (jnp.ones((TILES, 128), F32), jnp.zeros((TILES, 128), F32))
        before, before_d = run, run_d
        for o in range(NEAR):
            q = jnp.where(way == 0, o, NEAR - 1 - o)
            here = q == me
            before = tuple(jnp.where(here, a, b) for a, b in zip(run, before))
            before_d = tuple(jnp.where(here, a, b) for a, b in zip(run_d, before_d))
            gain = table_decay(way, tbuf[q])
            moved = times(*gain, *run)
            run = (moved[0] + sbuf[q, 0], moved[1] + sbuf[q, 1])
            run_d = times(*gain, *run_d)
        return before, before_d, run

    d_core().start()
    t_arrived("z", t_z, 9)
    mine = table_decay(way, t_own[...])
    d_core().wait_recv()
    moved = times(*mine, s_par[0], s_par[1])
    s_y[yi, 0] = moved[0] + ssum[way, 0]
    s_y[yi, 1] = moved[1] + ssum[way, 1]
    for c in d_stage("y", s_y, 1):
        c.start()

    def lead_in(tile, carry):
        for d in range(2):
            rate2, _, high, low, both = [
                jnp.broadcast_to(tabs[d, k, pl.ds(tile, 1), :], (SUBS, 128)) for k in range(5)
            ]
            g_re, g_im = stretch_decay(rate2, high, low, both, spans[0], spans[1])
            x_re, x_im = loc[tile, d, 0], loc[tile, d, 1]
            for hop in (1, 2, 4):
                turn = hop if d == 0 else SUBS - hop
                inside = sub8 >= hop if d == 0 else sub8 < SUBS - hop
                q_re, q_im, h_re, h_im = [pltpu.roll(v, turn, 0) for v in (x_re, x_im, g_re, g_im)]
                m_re, m_im = times(g_re, g_im, q_re, q_im)
                n_re, n_im = times(g_re, g_im, h_re, h_im)
                x_re, x_im = jnp.where(inside, x_re + m_re, x_re), jnp.where(inside, x_im + m_im, x_im)
                g_re, g_im = jnp.where(inside, n_re, g_re), jnp.where(inside, n_im, g_im)
            turn = 1 if d == 0 else SUBS - 1
            inside = sub8 >= 1 if d == 0 else sub8 < SUBS - 1
            x_re, x_im, g_re, g_im = [
                jnp.where(inside, pltpu.roll(v, turn, 0), blank_value)
                for v, blank_value in ((x_re, 0.0), (x_im, 0.0), (g_re, 1.0), (g_im, 0.0))
            ]
            lead[tile, d, 0] = x_re
            lead[tile, d, 1] = x_im
            fade[tile, d, 0] = g_re
            fade[tile, d, 1] = g_im
        return carry

    lax.fori_loop(0, TILES, lead_in, 0)

    c_sout.wait()
    lane_group = lax.broadcasted_iota(jnp.int32, (64, 128), 1) // 16
    blank = jnp.zeros((64, 128), BF16)

    def spread(m, carry):
        for d in range(2):
            for part in range(2):
                sign = 1.0 if part == 0 else -1.0
                at = (d * 2 + part) * 128
                lower = (sout_v[d, part, pl.ds(m * 8, 8)].reshape(128, 64) * sign).T
                upper = (sout_v[d, part, pl.ds(TILES + m * 8, 8)].reshape(128, 64) * sign).T
                for i in range(8):
                    tile = m * 8 + i
                    cst[tile, at:at + 64, 0:128] = jnp.where(lane_group == i, lower, 0.0).astype(BF16)
                    cst[tile, at:at + 64, 128:256] = blank
                    cst[tile, at + 64:at + 128, 0:128] = blank
                    cst[tile, at + 64:at + 128, 128:256] = jnp.where(lane_group == i, upper, 0.0).astype(BF16)
        return carry

    lax.fori_loop(0, 4, spread, 0)

    d_arrived("y", s_y, 1)
    y_in, y_fade, line_total = walk("y", s_y, t_y)
    s_x[xi, 0] = line_total[0]
    s_x[xi, 1] = line_total[1]
    for c in d_stage("x", s_x, 5):
        c.start()
    d_arrived("x", s_x, 5)
    x_in, x_fade, plane_total = walk("x", s_x, t_x)
    s_z[zi, 0] = plane_total[0]
    s_z[zi, 1] = plane_total[1]
    for c in d_stage("z", s_z, 9):
        c.start()
    both_fade = times(*y_fade, *x_fade)
    moved = times(*y_fade, *x_in)
    held = (moved[0] + y_in[0], moved[1] + y_in[1])
    other = table_decay(way, t_par[...])
    d_arrived("z", s_z, 9)
    z_in, _, _ = walk("z", s_z, t_z)
    moved = times(*both_fade, *z_in)
    chip = (moved[0] + held[0], moved[1] + held[1])
    s_fin[0] = chip[0]
    s_fin[1] = chip[1]
    last = pltpu.make_async_remote_copy(
        src_ref=s_fin, dst_ref=s_in, send_sem=d_send.at[13], recv_sem=d_recv.at[13],
        device_id=partner(), device_id_type=MESH,
    )
    last.start()
    moved = times(*other, *chip)
    ent[way, 0] = moved[0] + s_par[0]
    ent[way, 1] = moved[1] + s_par[1]
    last.wait_recv()
    ent[core, 0] = s_in[0]
    ent[core, 1] = s_in[1]

    def second_pass(tile, carry):
        parts = []
        for d in range(2):
            base = d * 256
            e_re = jnp.broadcast_to(ent[d, 0, pl.ds(tile, 1), :], (SUBS, 128))
            e_im = jnp.broadcast_to(ent[d, 1, pl.ds(tile, 1), :], (SUBS, 128))
            m_re, m_im = times(fade[tile, d, 0], fade[tile, d, 1], e_re, e_im)
            s_re, s_im = m_re + lead[tile, d, 0], m_im + lead[tile, d, 1]
            found = [None] * STEPS
            for j in range(STEPS) if d == 0 else range(STEPS - 1, -1, -1):
                at = pl.ds(j * SUBS, SUBS)
                n_re, n_im = times(dec[tile, at, base:base + 128], dec[tile, at, base + 128:base + 256], s_re, s_im)
                s_re = n_re + proj[tile, at, base:base + 128]
                s_im = n_im + proj[tile, at, base + 128:base + 256]
                found[j] = (s_re, s_im)
            for part in range(2):
                parts.append(jnp.concatenate([f[part] for f in found], axis=0).astype(BF16))
        states = jnp.concatenate(parts, axis=1)
        m = tile // 8
        resp[m] = resp[m] + jnp.dot(states, cst[tile], preferred_element_type=F32)
        return carry

    lax.fori_loop(0, TILES, second_pass, 0)

    c_gb.wait()
    c_glu.wait()
    response = jnp.concatenate(
        [resp[m, :, 0:128] for m in range(4)] + [resp[m, :, 128:256] for m in range(4)], axis=1
    )
    acc[...] = jax.nn.gelu(response, approximate=True)
    active_low = acc[...].astype(BF16)
    gates = []
    for n in range(4):
        at = slice(n * 256, (n + 1) * 256)
        gate = jnp.dot(active_low, glu_v[:, at], preferred_element_type=F32) + gbias_v[:, at]
        gates.append((acc[:, at] * jax.nn.sigmoid(gate)).astype(BF16))
    gated = jnp.dot(back, jnp.concatenate(gates, axis=1), preferred_element_type=F32).astype(BF16)
    c_og.wait()
    c_ow.wait()
    outs, square = [], None
    for n in range(8):
        at = slice(n * 256, (n + 1) * 256)
        piece = jnp.dot(gated, outw_v[:, at], preferred_element_type=F32)
        outs.append(piece)
        part = jnp.sum(piece * piece, axis=-1, keepdims=True)
        square = part if square is None else square + part
    scale = lax.rsqrt(square * (1.0 / 2048.0) + EPS)
    for n in range(8):
        at = slice(n * 256, (n + 1) * 256)
        out_ref[:, at] = (outs[n] * scale * ogain_v[:, at]).astype(BF16)

    t_core().wait_send()
    d_core().wait_send()
    for axis, tb, sb, base in (("y", t_y, s_y, 1), ("x", t_x, s_x, 5), ("z", t_z, s_z, 9)):
        for c in t_stage(axis, tb, base) + d_stage(axis, sb, base):
            c.wait_send()
    last.wait_send()


def local(
    tokens, elapsed, norm_gain, in_weight, state_input, state_output, forget_rate, decay_angle,
    skip_gain, glu_weight, glu_bias, out_weight, out_gain,
):
    args = (
        tokens, elapsed.reshape(1, -1), norm_gain.reshape(1, -1), in_weight, state_input.transpose(0, 1, 2, 4, 3),
        state_output, forget_rate, decay_angle, skip_gain.reshape(1, -1), glu_weight, glu_bias.reshape(1, -1),
        out_weight, out_gain.reshape(1, -1),
    )
    vm = pltpu.VMEM
    scratch = [vm(a.shape, a.dtype) for a in args]
    scratch += [
        vm((ROWS, 2048), BF16),
        vm((ROWS, 1024), F32),
        vm((4, ROWS, 256), BF16),
        vm((4, ROWS, 256), F32),
        vm((4, 256, 512), BF16),
        vm((TILES, 512, 256), BF16),
        vm((TILES, ROWS, 512), F32),
        vm((TILES, ROWS, 512), F32),
        vm((2, 5, TILES, 128), F32),
        vm((STEPS, SUBS, 128), F32),
        vm((6, SUBS, 128), F32),
        vm((TILES, 2, 2, SUBS, 128), F32),
        vm((2, 2, TILES, 128), F32),
        vm((TILES, 2, 2, SUBS, 128), F32),
        vm((TILES, 2, 2, SUBS, 128), F32),
        vm((2, 2, TILES, 128), F32),
        vm((8, 128), F32), vm((8, 128), F32),
        vm((4, 8, 128), F32), vm((4, 8, 128), F32), vm((4, 8, 128), F32),
        vm((2, TILES, 128), F32),
        vm((4, 2, TILES, 128), F32), vm((4, 2, TILES, 128), F32), vm((4, 2, TILES, 128), F32),
        vm((2, TILES, 128), F32), vm((2, TILES, 128), F32),
        pltpu.SemaphoreType.DMA((16,)),
        pltpu.SemaphoreType.DMA((14,)), pltpu.SemaphoreType.DMA((14,)),
        pltpu.SemaphoreType.DMA((14,)), pltpu.SemaphoreType.DMA((14,)),
    ]
    return pl.pallas_call(
        kernel,
        out_shape=jax.ShapeDtypeStruct(tokens.shape, BF16),
        in_specs=[pl.BlockSpec(memory_space=pl.ANY)] * len(args),
        out_specs=pl.BlockSpec(memory_space=pltpu.VMEM),
        scratch_shapes=scratch,
        compiler_params=pltpu.CompilerParams(
            collective_id=0, has_side_effects=True, vmem_limit_bytes=67000000
        ),
        name="ssm_layer",
    )(*args)


def solution(mesh):
    rows = P(("sp", "tp"), None)
    placed = (rows, P(("sp", "tp")), P(), P(), P(), P(), P(), P(), P(), P(), P(), P(), P())
    return jax.shard_map(local, mesh=mesh, in_specs=placed, out_specs=rows, check_vma=False)
```

```python
import functools
import math

import jax
import jax.numpy as jnp
from jax import lax
from jax.experimental import pallas as pl
from jax.experimental.pallas import tpu as pltpu
from jax.sharding import PartitionSpec as P

F32 = jnp.float32
BF16 = jnp.bfloat16
MESH = pl.DeviceIdType.MESH

ROWS = 128
TILES = 32
SUBS = 8
STEPS = 16
LINE = 8
LINES = 16
QUARTER = 8
EPS = 1e-06
LOG2E = 1.4426950408889634
SIN_C = (4.442883014678955, -7.308241367340088, 3.6062889099121094, -0.845763623714447, 0.10920575261116028)
COS_C = (1.4142135381698608, -6.9788641929626465, 5.73988151550293, -1.8882750272750854, 0.3322518765926361, -0.034502167254686356)
POINTS = [1.5 + 1.5 * math.cos((2 * i + 1) * math.pi / 32.0) for i in range(16)]
WEIGHTS = [1.0 / math.prod(p - o for o in POINTS if o != p) for p in POINTS]
INV_TURN = 1.0 / (2.0 * math.pi)
TURN_HI = math.floor(INV_TURN * 4096.0) / 4096.0
TURN_LO = INV_TURN - TURN_HI


def horner(x, coefficients):
    total = coefficients[-1]
    for c in coefficients[-2::-1]:
        total = total * x + c
    return total


def half_turn_parts(turns):
    part = turns - lax.round(turns, lax.RoundingMethod.TO_NEAREST_EVEN)
    square = part * part
    return part * horner(square, SIN_C), horner(square, COS_C)


def decay_parts(size, turns):
    sine, cosine = half_turn_parts(turns)
    lean = size * sine
    return size - lean * sine, lean * cosine


def in_parts(value, count):
    parts = []
    for _ in range(count):
        parts.append(value.astype(BF16))
        value = value - parts[-1].astype(F32)
    return parts


def times(a_re, a_im, b_re, b_im):
    return a_re * b_re - a_im * b_im, a_re * b_im + a_im * b_re


def kernel(
    tokens_h, elapsed_h, ngain_h, inw_h, sin_h, sout_h, rate_h, angle_h, skip_h, glu_h, gbias_h, outw_h, ogain_h,
    out_ref,
    tokens_v, elapsed_v, ngain_v, inw_v, sin_v, sout_v, rate_v, angle_v, skip_v, glu_v, gbias_v, outw_v, ogain_v,
    normed, acc, drv, resp, bst, cst, proj, dec, tabs, by_token, at_node, cell_decay, cell_gain, gain, states, spans, loc, ssum, lead, fade,
    t_dev, t_line, g_in, x_in, x_far, e_new, e_fade, e_in,
    dma_sem, t_send, t_recv, u_send, u_recv, g_send, g_recv, x_send, x_recv, e_send, e_recv,
):
    sp = lax.axis_index("sp")
    tp = lax.axis_index("tp")
    yi, core = tp // 2, tp % 2
    way = 1 - core

    def line_peer(k):
        return {"sp": sp, "tp": k}

    def plane_peer(k):
        return {"sp": k, "tp": tp}

    def remote(src, dst, send_sem, recv_sem, peer):
        return pltpu.make_async_remote_copy(
            src_ref=src, dst_ref=dst, send_sem=send_sem, recv_sem=recv_sem, device_id=peer, device_id_type=MESH,
        )

    def ahead(step):
        k = jnp.where(way == 0, sp + step, sp - step)
        return lax.rem(k + LINES, LINES), jnp.logical_and(k >= 0, k < LINES)

    def behind(step):
        return ahead(-step)

    pairs = [
        (elapsed_h, elapsed_v), (tokens_h, tokens_v), (ngain_h, ngain_v), (rate_h, rate_v), (angle_h, angle_v),
        (sin_h, sin_v), (sout_h, sout_v), (skip_h, skip_v), (gbias_h, gbias_v), (glu_h, glu_v),
        (ogain_h, ogain_v), (outw_h, outw_v),
    ]
    copies = [pltpu.make_async_copy(a, b, dma_sem.at[k]) for k, (a, b) in enumerate(pairs)]
    c_el, c_tok, c_ng, c_rate, c_ang, c_sin, c_sout, c_skip, c_gb, c_glu, c_og, c_ow = copies
    in_copies = [
        pltpu.make_async_copy(inw_h.at[pl.ds(k * 512, 512), :], inw_v.at[pl.ds(k * 512, 512), :], dma_sem.at[12 + k])
        for k in range(4)
    ]
    for c in (c_el, c_tok, c_ng, c_rate, c_ang):
        c.start()
    for c in in_copies:
        c.start()
    for c in (c_sin, c_sout, c_skip, c_gb, c_glu, c_og, c_ow):
        c.start()

    barrier = pltpu.get_barrier_semaphore()
    for k in range(1, LINE):
        pl.semaphore_signal(barrier, inc=1, device_id=line_peer(lax.rem(tp + k, LINE)), device_id_type=MESH)
    for k in range(1, LINES):
        pl.semaphore_signal(barrier, inc=1, device_id=plane_peer(lax.rem(sp + k, LINES)), device_id_type=MESH)

    c_el.wait()
    steps = elapsed_v[...]
    whole = jnp.floor(steps)
    rest = steps - whole
    lane8 = lax.broadcasted_iota(jnp.int32, (SUBS, 128), 1)
    sub8 = lax.broadcasted_iota(jnp.int32, (SUBS, 128), 0)

    def picked(mask, row):
        total = jnp.sum(jnp.where(mask, jnp.broadcast_to(row, (SUBS, 128)), 0.0), axis=1, keepdims=True)
        return jnp.broadcast_to(total, (SUBS, 128))

    t_dev[tp] = jnp.where(sub8 == 0, picked(lane8 >= 0, whole), picked(lane8 >= 0, rest))
    gaps = [steps - p for p in POINTS]
    upto, after = [jnp.ones_like(steps)], [jnp.ones_like(steps)]
    for k in range(15):
        upto.append(upto[-1] * gaps[k])
        after.append(after[-1] * gaps[15 - k])
    basis = [upto[k] * after[15 - k] * WEIGHTS[k] for k in range(16)]
    scale = basis[0]
    for b in basis[1:]:
        scale = scale + b
    basis = jnp.concatenate(basis, axis=0) / jnp.broadcast_to(scale, (16, 128))
    b1, b2, b3 = in_parts(basis, 3)
    r1, r2 = in_parts(basis * jnp.sqrt(steps), 2)
    none16 = jnp.zeros((16, 128), BF16)
    token_rows = jnp.concatenate([b1, b1, b2, b2, b1, b3, none16, none16], axis=0)
    gain_rows = jnp.concatenate([r1, r1, r2] + [none16] * 5, axis=0)
    row_i = lax.broadcasted_iota(jnp.int32, (ROWS, ROWS), 0)
    col_i = lax.broadcasted_iota(jnp.int32, (ROWS, ROWS), 1)
    order = jnp.where(col_i == (row_i % SUBS) * STEPS + row_i // SUBS, 1.0, 0.0).astype(BF16)
    back = jnp.where(row_i == (col_i % SUBS) * STEPS + col_i // SUBS, 1.0, 0.0).astype(BF16)
    across = (((1,), (1,)), ((), ()))
    for k, rows in enumerate((token_rows, gain_rows)):
        by_token[k] = lax.dot_general(order, rows, across, preferred_element_type=F32).astype(BF16)
    node_i = lax.broadcasted_iota(jnp.int32, (16, 128), 0)
    nodes = jnp.full((16, 128), POINTS[0], F32)
    for k in range(1, 16):
        nodes = jnp.where(node_i == k, POINTS[k], nodes)
    at_node[...] = nodes
    none32 = jnp.zeros((32, 512), BF16)
    none80 = jnp.zeros((80, 256), BF16)
    for t in range(QUARTER):
        cell_decay[t, 96:128, :] = none32
        cell_gain[t, 48:128, :] = none80
    stretch = lane8 // STEPS
    for k, mask in enumerate((stretch == sub8, stretch > sub8, stretch < sub8)):
        spans[2 * k] = picked(mask, whole)
        spans[2 * k + 1] = picked(mask, rest)

    def t_out(k):
        peer = lax.rem(tp + k, LINE)
        return remote(t_dev.at[tp], t_dev.at[tp], t_send.at[k], t_recv.at[tp], line_peer(peer))

    def t_in(k):
        peer = lax.rem(tp + k, LINE)
        return remote(t_dev.at[peer], t_dev.at[peer], t_send.at[k], t_recv.at[peer], line_peer(peer))

    def u_out(k, peer):
        return remote(t_line.at[sp], t_line.at[sp], u_send.at[k], u_recv.at[sp], plane_peer(peer))

    def u_in(k, peer):
        return remote(t_line.at[peer], t_line.at[peer], u_send.at[k], u_recv.at[peer], plane_peer(peer))

    def x_out(k, peer):
        return remote(x_in.at[sp], x_in.at[sp], x_send.at[k], x_recv.at[sp], plane_peer(peer))

    def x_arr(k, peer):
        return remote(x_in.at[peer], x_in.at[peer], x_send.at[k], x_recv.at[peer], plane_peer(peer))

    def g_out(d, q):
        return remote(ssum.at[d, q], g_in.at[tp], g_send.at[q * 2 + d], g_recv.at[tp], line_peer(q * 2 + 1 - d))

    def g_arr(k):
        peer = lax.rem(tp + k, LINE)
        return remote(ssum.at[0, 0], g_in.at[peer], g_send.at[k], g_recv.at[peer], line_peer(peer))

    def e_out(k):
        peer = lax.rem(tp + k, LINE)
        return remote(e_new.at[peer], e_in.at[tp], e_send.at[k], e_recv.at[tp], line_peer(peer))

    def e_arr(k):
        peer = lax.rem(tp + k, LINE)
        return remote(e_new.at[peer], e_in.at[peer], e_send.at[k], e_recv.at[peer], line_peer(peer))

    c_rate.wait()
    c_ang.wait()
    for d in range(2):
        rate = jnp.concatenate([rate_v[d, 0:TILES, :], rate_v[d, TILES:, :]], axis=1)
        angle = jnp.concatenate([angle_v[d, 0:TILES, :], angle_v[d, TILES:, :]], axis=1)
        tabs[d, 0] = rate * (-LOG2E)
        tabs[d, 1] = rate * 2.0
        big = lax.round(angle * 1024.0, lax.RoundingMethod.TO_NEAREST_EVEN) * (1.0 / 1024.0)
        small = angle - big
        first = big * TURN_HI
        second = big * TURN_LO + (small * TURN_HI + small * TURN_LO)
        high = lax.round(first * 256.0, lax.RoundingMethod.TO_NEAREST_EVEN) * (1.0 / 256.0)
        low = (first - high) + second
        tabs[d, 2] = high
        tabs[d, 3] = low
        tabs[d, 4] = high + low

    def stretch_decay(rate2, high, low, both, t_whole, t_rest):
        size = jnp.exp2(rate2 * (t_whole + t_rest))
        turns = high * t_whole
        turns = turns - lax.round(turns, lax.RoundingMethod.TO_NEAREST_EVEN)
        return decay_parts(size, turns + low * t_whole + both * t_rest)

    def quarter_decay(t_tile):
        t_whole = jnp.broadcast_to(t_tile[0:1, :], (QUARTER, 128))
        t_rest = jnp.broadcast_to(t_tile[1:2, :], (QUARTER, 128))
        rows = pl.ds(pl.multiple_of(yi * QUARTER, QUARTER), QUARTER)
        return stretch_decay(*[tabs[way, k, rows, :] for k in (0, 2, 3, 4)], t_whole, t_rest)

    c_tok.wait()
    c_ng.wait()
    for r in range(4):
        x = tokens_v[pl.ds(r * 32, 32), :].astype(F32)
        scale = lax.rsqrt(jnp.mean(x * x, axis=-1, keepdims=True) + EPS)
        normed[pl.ds(r * 32, 32), :] = (x * scale * ngain_v[...]).astype(BF16)

    for k in range(4):
        in_copies[k].wait()
        part = jnp.dot(normed[:, k * 512:(k + 1) * 512], inw_v[k * 512:(k + 1) * 512, :], preferred_element_type=F32)
        acc[...] = part if k == 0 else acc[...] + part

    driven = jnp.dot(order, acc[...].astype(BF16), preferred_element_type=F32)
    c_skip.wait()
    for m in range(4):
        low_d, high_d = driven[:, m * 128:(m + 1) * 128], driven[:, 512 + m * 128:512 + (m + 1) * 128]
        resp[m, :, 0:128] = low_d * skip_v[:, m * 128:(m + 1) * 128]
        resp[m, :, 128:256] = high_d * skip_v[:, 512 + m * 128:512 + (m + 1) * 128]
        drv[m, :, 0:128] = low_d.astype(BF16)
        drv[m, :, 128:256] = high_d.astype(BF16)

    pl.semaphore_wait(barrier, LINE - 1 + LINES - 1)
    for k in range(1, LINE):
        t_out(k).start()

    c_sin.wait()
    nothing = jnp.zeros((128, 64), BF16)
    for m in range(4):
        for d in range(2):
            for part in range(2):
                at = (d * 2 + part) * 128
                lower = sin_v[d, part, m * 8:(m + 1) * 8].reshape(128, 64)
                upper = sin_v[d, part, TILES + m * 8:TILES + (m + 1) * 8].reshape(128, 64)
                bst[m, 0:128, at:at + 128] = jnp.concatenate([lower, nothing], axis=1)
                bst[m, 128:256, at:at + 128] = jnp.concatenate([nothing, upper], axis=1)

    group_lane = (lax.broadcasted_iota(jnp.int32, (ROWS, 256), 1) // 16) % 8

    def first_pass(q, carry):
        def values_at_nodes(t):
            row = pl.ds(q * QUARTER + t, 1)
            x = at_node[...]
            for d in range(2):
                rate2, double, both = [jnp.broadcast_to(tabs[d, k, row, :], (16, 128)) for k in (0, 1, 4)]
                size = jnp.exp2(rate2 * x)
                y = double * x
                near = y * horner(y, (1.0, -0.5, 1.0 / 6.0, -1.0 / 24.0))
                gap = jnp.where(y < 0.03, near, 1.0 - size * size)
                for part, value in enumerate(decay_parts(size, both * x)):
                    v1, v2, v3 = in_parts(value, 3)
                    at = slice((d * 2 + part) * 128, (d * 2 + part + 1) * 128)
                    for k, v in enumerate((v1, v2, v1, v2, v3, v1)):
                        cell_decay[t, k * 16:(k + 1) * 16, at] = v
                g1, g2 = in_parts(gap * lax.rsqrt(jnp.maximum(gap * x, 1e-37)), 2)
                for k, v in enumerate((g1, g2, g1)):
                    cell_gain[t, k * 16:(k + 1) * 16, d * 128:(d + 1) * 128] = v

        def products(t):
            tile = q * QUARTER + t
            dec[tile] = jnp.dot(by_token[0], cell_decay[t], preferred_element_type=F32)
            gain[t] = jnp.dot(by_token[1], cell_gain[t], preferred_element_type=F32)
            lhs = drv[q] * jnp.where(group_lane == t, 1.0, 0.0).astype(BF16)
            proj[tile] = jnp.dot(lhs, bst[q], preferred_element_type=F32)

        def scan(t):
            tile = q * QUARTER + t
            for d in range(2):
                s_re = s_im = None
                base = d * 256
                for j in range(STEPS) if d == 0 else range(STEPS - 1, -1, -1):
                    at = pl.ds(j * SUBS, SUBS)
                    damp = gain[t, at, d * 128:(d + 1) * 128]
                    p_re = proj[tile, at, base:base + 128] * damp
                    p_im = proj[tile, at, base + 128:base + 256] * damp
                    proj[tile, at, base:base + 128] = p_re
                    proj[tile, at, base + 128:base + 256] = p_im
                    if s_re is None:
                        s_re, s_im = p_re, p_im
                    else:
                        a_re, a_im = dec[tile, at, base:base + 128], dec[tile, at, base + 128:base + 256]
                        n_re, n_im = times(a_re, a_im, s_re, s_im)
                        s_re, s_im = n_re + p_re, n_im + p_im
                loc[tile, d, 0] = s_re
                loc[tile, d, 1] = s_im
                k = 2 if d == 0 else 4
                rate2, high, low, both = [
                    jnp.broadcast_to(tabs[d, i, pl.ds(tile, 1), :], (SUBS, 128)) for i in (0, 2, 3, 4)
                ]
                w_re, w_im = stretch_decay(rate2, high, low, both, spans[k], spans[k + 1])
                m_re, m_im = times(w_re, w_im, s_re, s_im)
                ssum[d, q, 0, t:t + 1, :] = jnp.sum(m_re, axis=0, keepdims=True)
                ssum[d, q, 1, t:t + 1, :] = jnp.sum(m_im, axis=0, keepdims=True)

        @pl.when(q == 2)
        def _():
            for k in range(1, LINE):
                t_in(k).wait_recv()
            total = t_dev[0]
            for k in range(1, LINE):
                total = total + t_dev[k]
            t_line[sp] = total
            for k in range(1, LINES):
                peer, there = ahead(k)
                pl.when(there)(u_out(k, peer).start)

        values_at_nodes(0)
        products(0)
        values_at_nodes(1)
        for t in range(QUARTER):
            if t + 1 < QUARTER:
                products(t + 1)
            if t + 2 < QUARTER:
                values_at_nodes(t + 2)
            scan(t)
        for d in range(2):
            pl.when(tp != q * 2 + 1 - d)(g_out(d, q).start)
        return carry

    lax.fori_loop(0, TILES // QUARTER, first_pass, 0)

    def lead_in(tile, carry):
        for d in range(2):
            rate2, _, high, low, both = [
                jnp.broadcast_to(tabs[d, k, pl.ds(tile, 1), :], (SUBS, 128)) for k in range(5)
            ]
            g_re, g_im = stretch_decay(rate2, high, low, both, spans[0], spans[1])
            x_re, x_im = loc[tile, d, 0], loc[tile, d, 1]
            for hop in (1, 2, 4):
                turn = hop if d == 0 else SUBS - hop
                inside = sub8 >= hop if d == 0 else sub8 < SUBS - hop
                q_re, q_im, h_re, h_im = [pltpu.roll(v, turn, 0) for v in (x_re, x_im, g_re, g_im)]
                m_re, m_im = times(g_re, g_im, q_re, q_im)
                n_re, n_im = times(g_re, g_im, h_re, h_im)
                x_re, x_im = jnp.where(inside, x_re + m_re, x_re), jnp.where(inside, x_im + m_im, x_im)
                g_re, g_im = jnp.where(inside, n_re, g_re), jnp.where(inside, n_im, g_im)
            turn = 1 if d == 0 else SUBS - 1
            inside = sub8 >= 1 if d == 0 else sub8 < SUBS - 1
            x_re, x_im, g_re, g_im = [
                jnp.where(inside, pltpu.roll(v, turn, 0), blank_value)
                for v, blank_value in ((x_re, 0.0), (x_im, 0.0), (g_re, 1.0), (g_im, 0.0))
            ]
            lead[tile, d, 0] = x_re
            lead[tile, d, 1] = x_im
            fade[tile, d, 0] = g_re
            fade[tile, d, 1] = g_im
        return carry

    lax.fori_loop(0, TILES, lead_in, 0)

    c_sout.wait()
    lane_group = lax.broadcasted_iota(jnp.int32, (64, 128), 1) // 16
    blank = jnp.zeros((64, 128), BF16)

    def spread(m, carry):
        for d in range(2):
            for part in range(2):
                sign = 1.0 if part == 0 else -1.0
                at = (d * 2 + part) * 128
                lower = (sout_v[d, part, pl.ds(m * 8, 8)].reshape(128, 64) * sign).T
                upper = (sout_v[d, part, pl.ds(TILES + m * 8, 8)].reshape(128, 64) * sign).T
                for i in range(8):
                    tile = m * 8 + i
                    cst[tile, at:at + 64, 0:128] = jnp.where(lane_group == i, lower, 0.0).astype(BF16)
                    cst[tile, at:at + 64, 128:256] = blank
                    cst[tile, at + 64:at + 128, 0:128] = blank
                    cst[tile, at + 64:at + 128, 128:256] = jnp.where(lane_group == i, upper, 0.0).astype(BF16)
        return carry

    lax.fori_loop(0, 4, spread, 0)

    g_in[tp] = ssum[way, yi]
    for k in range(1, LINES):
        peer, there = behind(k)
        pl.when(there)(u_in(k, peer).wait_recv)
    places = [jnp.where(way == 0, o, LINE - 1 - o) for o in range(LINE)]
    gains = [quarter_decay(t_dev[k]) for k in places]
    for k in range(1, LINE):
        g_arr(k).wait_recv()
    zero, one = jnp.zeros((QUARTER, 128), F32), jnp.ones((QUARTER, 128), F32)
    run, run_d, before, before_d = (zero, zero), (one, zero), [], []
    for o, k in enumerate(places):
        before.append(run)
        before_d.append(run_d)
        moved = times(*gains[o], *run)
        run = (moved[0] + g_in[k, 0], moved[1] + g_in[k, 1])
        run_d = times(*gains[o], *run_d)
    x_in[sp, 0] = run[0]
    x_in[sp, 1] = run[1]
    for k in range(1, LINES):
        peer, there = ahead(k)
        pl.when(there)(x_out(k, peer).start)
    for o, k in enumerate(places):
        e_new[k, 0] = before[o][0]
        e_new[k, 1] = before[o][1]
        e_fade[k, 0] = before_d[o][0]
        e_fade[k, 1] = before_d[o][1]
    between = jnp.zeros((SUBS, 128), F32)
    for k in range(1, LINES):
        peer, there = behind(k)
        far_re, far_im = quarter_decay(between)
        x_far[k, 0] = far_re
        x_far[k, 1] = far_im
        between = between + jnp.where(there, t_line[peer], 0.0)

    def local_pass(q, carry):
        total = resp[q]
        for t in range(QUARTER):
            tile = q * QUARTER + t
            for d in range(2):
                base = d * 256
                s_re, s_im = lead[tile, d, 0], lead[tile, d, 1]
                f_re, f_im = fade[tile, d, 0], fade[tile, d, 1]
                found = [None] * STEPS
                for j in range(STEPS) if d == 0 else range(STEPS - 1, -1, -1):
                    at = pl.ds(j * SUBS, SUBS)
                    a_re, a_im = dec[tile, at, base:base + 128], dec[tile, at, base + 128:base + 256]
                    n_re, n_im = times(a_re, a_im, s_re, s_im)
                    s_re = n_re + proj[tile, at, base:base + 128]
                    s_im = n_im + proj[tile, at, base + 128:base + 256]
                    f_re, f_im = times(a_re, a_im, f_re, f_im)
                    dec[tile, at, base:base + 128] = f_re
                    dec[tile, at, base + 128:base + 256] = f_im
                    found[j] = (s_re, s_im)
                    if j % 2 == (1 if d == 0 else 0):
                        first = j - j % 2
                        for part in range(2):
                            pair = jnp.concatenate([found[first][part], found[first + 1][part]], axis=0)
                            states[t, first * SUBS:(first + 2) * SUBS, base + part * 128:base + part * 128 + 128] = (
                                pair.astype(BF16)
                            )
            if t:
                total = total + jnp.dot(states[t - 1], cst[tile - 1], preferred_element_type=F32)
        resp[q] = total + jnp.dot(states[QUARTER - 1], cst[q * QUARTER + QUARTER - 1], preferred_element_type=F32)
        return carry

    lax.fori_loop(0, TILES // QUARTER, local_pass, 0)

    gone = (zero, zero)
    for k in range(1, LINES):
        peer, there = behind(k)
        pl.when(there)(x_arr(k, peer).wait_recv)
        moved = times(x_far[k, 0], x_far[k, 1], x_in[peer, 0], x_in[peer, 1])
        gone = tuple(g + jnp.where(there, m, 0.0) for g, m in zip(gone, moved))
    for k in range(LINE):
        moved = times(e_fade[k, 0], e_fade[k, 1], *gone)
        e_new[k, 0] = e_new[k, 0] + moved[0]
        e_new[k, 1] = e_new[k, 1] + moved[1]
    for k in range(1, LINE):
        e_out(k).start()
    e_in[tp] = e_new[tp]
    for k in range(1, LINE):
        e_arr(k).wait_recv()

    def second_pass(q, carry):
        total = resp[q]
        for t in range(QUARTER):
            tile = q * QUARTER + t
            for d in range(2):
                base = d * 256
                e_re = jnp.broadcast_to(e_in[q * 2 + 1 - d, 0, t:t + 1, :], (16, 128))
                e_im = jnp.broadcast_to(e_in[q * 2 + 1 - d, 1, t:t + 1, :], (16, 128))
                for r in range(0, ROWS, 16):
                    f_re, f_im = dec[tile, r:r + 16, base:base + 128], dec[tile, r:r + 16, base + 128:base + 256]
                    m_re, m_im = times(f_re, f_im, e_re, e_im)
                    states[t, r:r + 16, base:base + 128] = m_re.astype(BF16)
                    states[t, r:r + 16, base + 128:base + 256] = m_im.astype(BF16)
            if t:
                total = total + jnp.dot(states[t - 1], cst[tile - 1], preferred_element_type=F32)
        resp[q] = total + jnp.dot(states[QUARTER - 1], cst[q * QUARTER + QUARTER - 1], preferred_element_type=F32)
        return carry

    lax.fori_loop(0, TILES // QUARTER, second_pass, 0)

    c_gb.wait()
    c_glu.wait()
    response = jnp.concatenate(
        [resp[m, :, 0:128] for m in range(4)] + [resp[m, :, 128:256] for m in range(4)], axis=1
    )
    acc[...] = jax.nn.gelu(response, approximate=True)
    active_low = acc[...].astype(BF16)
    gates = []
    for n in range(4):
        at = slice(n * 256, (n + 1) * 256)
        gate = jnp.dot(active_low, glu_v[:, at], preferred_element_type=F32) + gbias_v[:, at]
        gates.append((acc[:, at] * jax.nn.sigmoid(gate)).astype(BF16))
    gated = jnp.dot(back, jnp.concatenate(gates, axis=1), preferred_element_type=F32).astype(BF16)
    c_og.wait()
    c_ow.wait()
    outs, square = [], None
    for n in range(8):
        at = slice(n * 256, (n + 1) * 256)
        piece = jnp.dot(gated, outw_v[:, at], preferred_element_type=F32)
        outs.append(piece)
        part = jnp.sum(piece * piece, axis=-1, keepdims=True)
        square = part if square is None else square + part
    scale = lax.rsqrt(square * (1.0 / 2048.0) + EPS)
    for n in range(8):
        at = slice(n * 256, (n + 1) * 256)
        out_ref[:, at] = (outs[n] * scale * ogain_v[:, at]).astype(BF16)

    for k in range(1, LINE):
        t_out(k).wait_send()
        e_out(k).wait_send()
    for q in range(TILES // QUARTER):
        for d in range(2):
            pl.when(tp != q * 2 + 1 - d)(g_out(d, q).wait_send)
    for k in range(1, LINES):
        peer, there = ahead(k)
        pl.when(there)(u_out(k, peer).wait_send)
        pl.when(there)(x_out(k, peer).wait_send)


def local(
    tokens, elapsed, norm_gain, in_weight, state_input, state_output, forget_rate, decay_angle,
    skip_gain, glu_weight, glu_bias, out_weight, out_gain,
):
    args = (
        tokens, elapsed.reshape(1, -1), norm_gain.reshape(1, -1), in_weight, state_input.transpose(0, 1, 2, 4, 3),
        state_output, forget_rate, decay_angle, skip_gain.reshape(1, -1), glu_weight, glu_bias.reshape(1, -1),
        out_weight, out_gain.reshape(1, -1),
    )
    vm = pltpu.VMEM
    scratch = [vm(a.shape, a.dtype) for a in args]
    scratch += [
        vm((ROWS, 2048), BF16),
        vm((ROWS, 1024), F32),
        vm((4, ROWS, 256), BF16),
        vm((4, ROWS, 256), F32),
        vm((4, 256, 512), BF16),
        vm((TILES, 512, 256), BF16),
        vm((TILES, ROWS, 512), F32),
        vm((TILES, ROWS, 512), F32),
        vm((2, 5, TILES, 128), F32),
        vm((2, ROWS, 128), BF16),
        vm((16, 128), F32),
        vm((QUARTER, 128, 512), BF16),
        vm((QUARTER, 128, 256), BF16),
        vm((QUARTER, ROWS, 256), F32),
        vm((QUARTER, ROWS, 512), BF16),
        vm((6, SUBS, 128), F32),
        vm((TILES, 2, 2, SUBS, 128), F32),
        vm((2, 4, 2, QUARTER, 128), F32),
        vm((TILES, 2, 2, SUBS, 128), F32),
        vm((TILES, 2, 2, SUBS, 128), F32),
        vm((LINE, SUBS, 128), F32),
        vm((LINES, SUBS, 128), F32),
        vm((LINE, 2, QUARTER, 128), F32),
        vm((LINES, 2, QUARTER, 128), F32),
        vm((LINES, 2, QUARTER, 128), F32),
        vm((LINE, 2, QUARTER, 128), F32),
        vm((LINE, 2, QUARTER, 128), F32),
        vm((LINE, 2, QUARTER, 128), F32),
        pltpu.SemaphoreType.DMA((16,)),
    ]
    for count in (LINE, LINES, LINE, LINES, LINE):
        scratch += [pltpu.SemaphoreType.DMA((count,)), pltpu.SemaphoreType.DMA((count,))]
    return pl.pallas_call(
        kernel,
        out_shape=jax.ShapeDtypeStruct(tokens.shape, BF16),
        in_specs=[pl.BlockSpec(memory_space=pl.ANY)] * len(args),
        out_specs=pl.BlockSpec(memory_space=pltpu.VMEM),
        scratch_shapes=scratch,
        compiler_params=pltpu.CompilerParams(
            collective_id=0, has_side_effects=True, vmem_limit_bytes=67000000
        ),
        name="ssm_layer",
    )(*args)


def solution(mesh):
    rows = P(("sp", "tp"), None)
    placed = (rows, P(("sp", "tp")), P(), P(), P(), P(), P(), P(), P(), P(), P(), P(), P())
    return jax.shard_map(local, mesh=mesh, in_specs=placed, out_specs=rows, check_vma=False)
```

```python
import functools
import math

import jax
import jax.numpy as jnp
from jax import lax
from jax.experimental import pallas as pl
from jax.experimental.pallas import tpu as pltpu
from jax.sharding import PartitionSpec as P

F32 = jnp.float32
BF16 = jnp.bfloat16
MESH = pl.DeviceIdType.MESH

ROWS = 128
TILES = 32
SUBS = 8
STEPS = 16
LINE = 8
LINES = 16
QUARTER = 8
EPS = 1e-06
LOG2E = 1.4426950408889634
SIN_C = (4.442883014678955, -7.308241367340088, 3.6062889099121094, -0.845763623714447, 0.10920575261116028)
COS_C = (1.4142135381698608, -6.9788641929626465, 5.73988151550293, -1.8882750272750854, 0.3322518765926361, -0.034502167254686356)
POINTS = [1.5 + 1.5 * math.cos((2 * i + 1) * math.pi / 32.0) for i in range(16)]
WEIGHTS = [1.0 / math.prod(p - o for o in POINTS if o != p) for p in POINTS]
INV_TURN = 1.0 / (2.0 * math.pi)
TURN_HI = math.floor(INV_TURN * 4096.0) / 4096.0
TURN_LO = INV_TURN - TURN_HI


def horner(x, coefficients):
    total = coefficients[-1]
    for c in coefficients[-2::-1]:
        total = total * x + c
    return total


def half_turn_parts(turns):
    part = turns - lax.round(turns, lax.RoundingMethod.TO_NEAREST_EVEN)
    square = part * part
    return part * horner(square, SIN_C), horner(square, COS_C)


def decay_parts(size, turns):
    sine, cosine = half_turn_parts(turns)
    lean = size * sine
    return size - lean * sine, lean * cosine


def in_parts(value, count):
    parts = []
    for _ in range(count):
        parts.append(value.astype(BF16))
        value = value - parts[-1].astype(F32)
    return parts


def times(a_re, a_im, b_re, b_im):
    return a_re * b_re - a_im * b_im, a_re * b_im + a_im * b_re


def kernel(
    tokens_h, elapsed_h, ngain_h, inw_h, sin_h, sout_h, rate_h, angle_h, skip_h, glu_h, outw_h,
    resp, glu_v, outw_v,
    tokens_v, elapsed_v, ngain_v, inw_v, sin_v, sout_v, rate_v, angle_v, skip_v,
    normed, acc, drv, bst, cst, proj, dec, tabs, by_token, at_node, cell_decay, cell_gain, gain, states, spans, loc, ssum, lead, fade,
    t_dev, t_line, g_in, x_in, x_far, e_new, e_fade, e_in,
    dma_sem, t_send, t_recv, u_send, u_recv, g_send, g_recv, x_send, x_recv, e_send, e_recv,
):
    sp = lax.axis_index("sp")
    tp = lax.axis_index("tp")
    yi, core = tp // 2, tp % 2
    way = core

    def line_peer(k):
        return {"sp": sp, "tp": k}

    def plane_peer(k):
        return {"sp": k, "tp": tp}

    def remote(src, dst, send_sem, recv_sem, peer):
        return pltpu.make_async_remote_copy(
            src_ref=src, dst_ref=dst, send_sem=send_sem, recv_sem=recv_sem, device_id=peer, device_id_type=MESH,
        )

    def ahead(step):
        k = jnp.where(way == 0, sp + step, sp - step)
        return lax.rem(k + LINES, LINES), jnp.logical_and(k >= 0, k < LINES)

    def behind(step):
        return ahead(-step)

    pairs = [
        (elapsed_h, elapsed_v), (tokens_h, tokens_v), (ngain_h, ngain_v), (rate_h, rate_v), (angle_h, angle_v),
        (sin_h, sin_v), (sout_h, sout_v), (skip_h, skip_v), (glu_h, glu_v), (outw_h, outw_v),
    ]
    copies = [pltpu.make_async_copy(a, b, dma_sem.at[k]) for k, (a, b) in enumerate(pairs)]
    c_el, c_tok, c_ng, c_rate, c_ang, c_sin, c_sout, c_skip, c_glu, c_ow = copies
    in_copies = [
        pltpu.make_async_copy(inw_h.at[pl.ds(k * 512, 512), :], inw_v.at[pl.ds(k * 512, 512), :], dma_sem.at[12 + k])
        for k in range(4)
    ]
    for c in (c_el, c_tok, c_ng, c_rate, c_ang):
        c.start()
    for c in in_copies:
        c.start()
    for c in (c_sin, c_sout, c_skip, c_glu, c_ow):
        c.start()

    barrier = pltpu.get_barrier_semaphore()
    for k in range(1, LINE):
        pl.semaphore_signal(barrier, inc=1, device_id=line_peer(lax.rem(tp + k, LINE)), device_id_type=MESH)
    for k in range(1, LINES):
        pl.semaphore_signal(barrier, inc=1, device_id=plane_peer(lax.rem(sp + k, LINES)), device_id_type=MESH)

    c_el.wait()
    steps = elapsed_v[...]
    whole = jnp.floor(steps)
    rest = steps - whole
    lane8 = lax.broadcasted_iota(jnp.int32, (SUBS, 128), 1)
    sub8 = lax.broadcasted_iota(jnp.int32, (SUBS, 128), 0)

    def picked(mask, row):
        total = jnp.sum(jnp.where(mask, jnp.broadcast_to(row, (SUBS, 128)), 0.0), axis=1, keepdims=True)
        return jnp.broadcast_to(total, (SUBS, 128))

    t_dev[tp] = jnp.where(sub8 == 0, picked(lane8 >= 0, whole), picked(lane8 >= 0, rest))
    gaps = [steps - p for p in POINTS]
    upto, after = [jnp.ones_like(steps)], [jnp.ones_like(steps)]
    for k in range(15):
        upto.append(upto[-1] * gaps[k])
        after.append(after[-1] * gaps[15 - k])
    basis = [upto[k] * after[15 - k] * WEIGHTS[k] for k in range(16)]
    scale = basis[0]
    for b in basis[1:]:
        scale = scale + b
    basis = jnp.concatenate(basis, axis=0) / jnp.broadcast_to(scale, (16, 128))
    b1, b2, b3 = in_parts(basis, 3)
    r1, r2 = in_parts(basis * jnp.sqrt(steps), 2)
    none16 = jnp.zeros((16, 128), BF16)
    token_rows = jnp.concatenate([b1, b1, b2, b2, b1, b3, none16, none16], axis=0)
    gain_rows = jnp.concatenate([r1, r1, r2] + [none16] * 5, axis=0)
    row_i = lax.broadcasted_iota(jnp.int32, (ROWS, ROWS), 0)
    col_i = lax.broadcasted_iota(jnp.int32, (ROWS, ROWS), 1)
    order = jnp.where(col_i == (row_i % SUBS) * STEPS + row_i // SUBS, 1.0, 0.0).astype(BF16)
    across = (((1,), (1,)), ((), ()))
    for k, rows in enumerate((token_rows, gain_rows)):
        by_token[k] = lax.dot_general(order, rows, across, preferred_element_type=F32).astype(BF16)
    node_i = lax.broadcasted_iota(jnp.int32, (16, 128), 0)
    nodes = jnp.full((16, 128), POINTS[0], F32)
    for k in range(1, 16):
        nodes = jnp.where(node_i == k, POINTS[k], nodes)
    at_node[...] = nodes
    none32 = jnp.zeros((32, 512), BF16)
    none80 = jnp.zeros((80, 256), BF16)
    for t in range(QUARTER):
        cell_decay[t, 96:128, :] = none32
        cell_gain[t, 48:128, :] = none80
    stretch = lane8 // STEPS
    for k, mask in enumerate((stretch == sub8, stretch > sub8, stretch < sub8)):
        spans[2 * k] = picked(mask, whole)
        spans[2 * k + 1] = picked(mask, rest)

    def t_out(k):
        peer = lax.rem(tp + k, LINE)
        return remote(t_dev.at[tp], t_dev.at[tp], t_send.at[k], t_recv.at[tp], line_peer(peer))

    def t_in(k):
        peer = lax.rem(tp + k, LINE)
        return remote(t_dev.at[peer], t_dev.at[peer], t_send.at[k], t_recv.at[peer], line_peer(peer))

    def u_out(k, peer):
        return remote(t_line.at[sp], t_line.at[sp], u_send.at[k], u_recv.at[sp], plane_peer(peer))

    def u_in(k, peer):
        return remote(t_line.at[peer], t_line.at[peer], u_send.at[k], u_recv.at[peer], plane_peer(peer))

    def x_out(k, peer):
        return remote(x_in.at[sp], x_in.at[sp], x_send.at[k], x_recv.at[sp], plane_peer(peer))

    def x_arr(k, peer):
        return remote(x_in.at[peer], x_in.at[peer], x_send.at[k], x_recv.at[peer], plane_peer(peer))

    def g_out(d, q):
        return remote(ssum.at[d, q], g_in.at[tp], g_send.at[q * 2 + d], g_recv.at[tp], line_peer(q * 2 + d))

    def g_arr(k):
        peer = lax.rem(tp + k, LINE)
        return remote(ssum.at[0, 0], g_in.at[peer], g_send.at[k], g_recv.at[peer], line_peer(peer))

    def e_out(k):
        peer = lax.rem(tp + k, LINE)
        return remote(e_new.at[peer], e_in.at[tp], e_send.at[k], e_recv.at[tp], line_peer(peer))

    def e_arr(k):
        peer = lax.rem(tp + k, LINE)
        return remote(e_new.at[peer], e_in.at[peer], e_send.at[k], e_recv.at[peer], line_peer(peer))

    c_rate.wait()
    c_ang.wait()
    for d in range(2):
        rate = jnp.concatenate([rate_v[d, 0:TILES, :], rate_v[d, TILES:, :]], axis=1)
        angle = jnp.concatenate([angle_v[d, 0:TILES, :], angle_v[d, TILES:, :]], axis=1)
        tabs[d, 0] = rate * (-LOG2E)
        tabs[d, 1] = rate * 2.0
        big = lax.round(angle * 1024.0, lax.RoundingMethod.TO_NEAREST_EVEN) * (1.0 / 1024.0)
        small = angle - big
        first = big * TURN_HI
        second = big * TURN_LO + (small * TURN_HI + small * TURN_LO)
        high = lax.round(first * 256.0, lax.RoundingMethod.TO_NEAREST_EVEN) * (1.0 / 256.0)
        low = (first - high) + second
        tabs[d, 2] = high
        tabs[d, 3] = low
        tabs[d, 4] = high + low

    def stretch_decay(rate2, high, low, both, t_whole, t_rest):
        size = jnp.exp2(rate2 * (t_whole + t_rest))
        turns = high * t_whole
        turns = turns - lax.round(turns, lax.RoundingMethod.TO_NEAREST_EVEN)
        return decay_parts(size, turns + low * t_whole + both * t_rest)

    def quarter_decay(t_tile):
        t_whole = jnp.broadcast_to(t_tile[0:1, :], (QUARTER, 128))
        t_rest = jnp.broadcast_to(t_tile[1:2, :], (QUARTER, 128))
        rows = pl.ds(pl.multiple_of(yi * QUARTER, QUARTER), QUARTER)
        return stretch_decay(*[tabs[way, k, rows, :] for k in (0, 2, 3, 4)], t_whole, t_rest)

    c_tok.wait()
    c_ng.wait()
    for r in range(4):
        x = tokens_v[pl.ds(r * 32, 32), :].astype(F32)
        scale = lax.rsqrt(jnp.mean(x * x, axis=-1, keepdims=True) + EPS)
        normed[pl.ds(r * 32, 32), :] = (x * scale * ngain_v[...]).astype(BF16)

    for k in range(4):
        in_copies[k].wait()
        part = jnp.dot(normed[:, k * 512:(k + 1) * 512], inw_v[k * 512:(k + 1) * 512, :], preferred_element_type=F32)
        acc[...] = part if k == 0 else acc[...] + part

    driven = jnp.dot(order, acc[...].astype(BF16), preferred_element_type=F32)
    c_skip.wait()
    for m in range(4):
        low_d, high_d = driven[:, m * 128:(m + 1) * 128], driven[:, 512 + m * 128:512 + (m + 1) * 128]
        resp[m, :, 0:128] = low_d * skip_v[:, m * 128:(m + 1) * 128]
        resp[m, :, 128:256] = high_d * skip_v[:, 512 + m * 128:512 + (m + 1) * 128]
        drv[m, :, 0:128] = low_d.astype(BF16)
        drv[m, :, 128:256] = high_d.astype(BF16)

    c_sin.wait()
    nothing = jnp.zeros((128, 64), BF16)
    for m in range(4):
        for d in range(2):
            for part in range(2):
                at = (d * 2 + part) * 128
                lower = sin_v[d, part, m * 8:(m + 1) * 8].reshape(128, 64)
                upper = sin_v[d, part, TILES + m * 8:TILES + (m + 1) * 8].reshape(128, 64)
                bst[m, 0:128, at:at + 128] = jnp.concatenate([lower, nothing], axis=1)
                bst[m, 128:256, at:at + 128] = jnp.concatenate([nothing, upper], axis=1)

    group_lane = (lax.broadcasted_iota(jnp.int32, (ROWS, 256), 1) // 16) % 8

    def first_pass(q, carry):
        def values_at_nodes(t):
            row = pl.ds(q * QUARTER + t, 1)
            x = at_node[...]
            for d in range(2):
                rate2, double, both = [jnp.broadcast_to(tabs[d, k, row, :], (16, 128)) for k in (0, 1, 4)]
                size = jnp.exp2(rate2 * x)
                y = double * x
                near = y * horner(y, (1.0, -0.5, 1.0 / 6.0, -1.0 / 24.0))
                gap = jnp.where(y < 0.03, near, 1.0 - size * size)
                for part, value in enumerate(decay_parts(size, both * x)):
                    v1, v2, v3 = in_parts(value, 3)
                    at = slice((d * 2 + part) * 128, (d * 2 + part + 1) * 128)
                    for k, v in enumerate((v1, v2, v1, v2, v3, v1)):
                        cell_decay[t, k * 16:(k + 1) * 16, at] = v
                g1, g2 = in_parts(gap * lax.rsqrt(jnp.maximum(gap * x, 1e-37)), 2)
                for k, v in enumerate((g1, g2, g1)):
                    cell_gain[t, k * 16:(k + 1) * 16, d * 128:(d + 1) * 128] = v

        def products(t):
            tile = q * QUARTER + t
            dec[tile] = jnp.dot(by_token[0], cell_decay[t], preferred_element_type=F32)
            gain[t] = jnp.dot(by_token[1], cell_gain[t], preferred_element_type=F32)
            lhs = drv[q] * jnp.where(group_lane == t, 1.0, 0.0).astype(BF16)
            proj[tile] = jnp.dot(lhs, bst[q], preferred_element_type=F32)

        def scan(t):
            tile = q * QUARTER + t
            for d in range(2):
                s_re = s_im = None
                base = d * 256
                for j in range(STEPS) if d == 0 else range(STEPS - 1, -1, -1):
                    at = pl.ds(j * SUBS, SUBS)
                    damp = gain[t, at, d * 128:(d + 1) * 128]
                    p_re = proj[tile, at, base:base + 128] * damp
                    p_im = proj[tile, at, base + 128:base + 256] * damp
                    proj[tile, at, base:base + 128] = p_re
                    proj[tile, at, base + 128:base + 256] = p_im
                    if s_re is None:
                        s_re, s_im = p_re, p_im
                    else:
                        a_re, a_im = dec[tile, at, base:base + 128], dec[tile, at, base + 128:base + 256]
                        n_re, n_im = times(a_re, a_im, s_re, s_im)
                        s_re, s_im = n_re + p_re, n_im + p_im
                loc[tile, d, 0] = s_re
                loc[tile, d, 1] = s_im
                k = 2 if d == 0 else 4
                rate2, high, low, both = [
                    jnp.broadcast_to(tabs[d, i, pl.ds(tile, 1), :], (SUBS, 128)) for i in (0, 2, 3, 4)
                ]
                w_re, w_im = stretch_decay(rate2, high, low, both, spans[k], spans[k + 1])
                m_re, m_im = times(w_re, w_im, s_re, s_im)
                ssum[d, q, 0, t:t + 1, :] = jnp.sum(m_re, axis=0, keepdims=True)
                ssum[d, q, 1, t:t + 1, :] = jnp.sum(m_im, axis=0, keepdims=True)

        @pl.when(q == 1)
        def _():
            pl.semaphore_wait(barrier, LINE - 1 + LINES - 1)
            for k in range(1, LINE):
                t_out(k).start()

        @pl.when(q > 0)
        def _():
            for d in range(2):
                pl.when(tp != (q - 1) * 2 + d)(g_out(d, q - 1).start)

        values_at_nodes(0)
        products(0)
        values_at_nodes(1)
        for t in range(QUARTER):
            if t + 1 < QUARTER:
                products(t + 1)
            if t + 2 < QUARTER:
                values_at_nodes(t + 2)
            scan(t)
        return carry

    lax.fori_loop(0, TILES // QUARTER, first_pass, 0)
    for d in range(2):
        pl.when(tp != LINE - 2 + d)(g_out(d, TILES // QUARTER - 1).start)

    def lead_in(tile, carry):
        for d in range(2):
            rate2, _, high, low, both = [
                jnp.broadcast_to(tabs[d, k, pl.ds(tile, 1), :], (SUBS, 128)) for k in range(5)
            ]
            g_re, g_im = stretch_decay(rate2, high, low, both, spans[0], spans[1])
            x_re, x_im = loc[tile, d, 0], loc[tile, d, 1]
            for hop in (1, 2, 4):
                turn = hop if d == 0 else SUBS - hop
                inside = sub8 >= hop if d == 0 else sub8 < SUBS - hop
                q_re, q_im, h_re, h_im = [pltpu.roll(v, turn, 0) for v in (x_re, x_im, g_re, g_im)]
                m_re, m_im = times(g_re, g_im, q_re, q_im)
                n_re, n_im = times(g_re, g_im, h_re, h_im)
                x_re, x_im = jnp.where(inside, x_re + m_re, x_re), jnp.where(inside, x_im + m_im, x_im)
                g_re, g_im = jnp.where(inside, n_re, g_re), jnp.where(inside, n_im, g_im)
            turn = 1 if d == 0 else SUBS - 1
            inside = sub8 >= 1 if d == 0 else sub8 < SUBS - 1
            x_re, x_im, g_re, g_im = [
                jnp.where(inside, pltpu.roll(v, turn, 0), blank_value)
                for v, blank_value in ((x_re, 0.0), (x_im, 0.0), (g_re, 1.0), (g_im, 0.0))
            ]
            lead[tile, d, 0] = x_re
            lead[tile, d, 1] = x_im
            fade[tile, d, 0] = g_re
            fade[tile, d, 1] = g_im
        return carry

    lax.fori_loop(0, TILES, lead_in, 0)

    for k in range(1, LINE):
        t_in(k).wait_recv()
    total = t_dev[0]
    for k in range(1, LINE):
        total = total + t_dev[k]
    t_line[sp] = total
    for k in range(1, LINES):
        peer, there = ahead(k)
        pl.when(there)(u_out(k, peer).start)

    c_sout.wait()
    lane_group = lax.broadcasted_iota(jnp.int32, (64, 128), 1) // 16
    blank = jnp.zeros((64, 128), BF16)

    def spread(m, carry):
        for d in range(2):
            for part in range(2):
                sign = 1.0 if part == 0 else -1.0
                at = (d * 2 + part) * 128
                lower = (sout_v[d, part, pl.ds(m * 8, 8)].reshape(128, 64) * sign).T
                upper = (sout_v[d, part, pl.ds(TILES + m * 8, 8)].reshape(128, 64) * sign).T
                for i in range(8):
                    tile = m * 8 + i
                    cst[tile, at:at + 64, 0:128] = jnp.where(lane_group == i, lower, 0.0).astype(BF16)
                    cst[tile, at:at + 64, 128:256] = blank
                    cst[tile, at + 64:at + 128, 0:128] = blank
                    cst[tile, at + 64:at + 128, 128:256] = jnp.where(lane_group == i, upper, 0.0).astype(BF16)
        return carry

    lax.fori_loop(0, 4, spread, 0)

    g_in[tp] = ssum[way, yi]
    places = [jnp.where(way == 0, o, LINE - 1 - o) for o in range(LINE)]
    gains = [quarter_decay(t_dev[k]) for k in places]
    for k in range(1, LINE):
        g_arr(k).wait_recv()
    zero, one = jnp.zeros((QUARTER, 128), F32), jnp.ones((QUARTER, 128), F32)
    run, run_d, before, before_d = (zero, zero), (one, zero), [], []
    for o, k in enumerate(places):
        before.append(run)
        before_d.append(run_d)
        moved = times(*gains[o], *run)
        run = (moved[0] + g_in[k, 0], moved[1] + g_in[k, 1])
        run_d = times(*gains[o], *run_d)
    x_in[sp, 0] = run[0]
    x_in[sp, 1] = run[1]
    for k in range(1, LINES):
        peer, there = ahead(k)
        pl.when(there)(x_out(k, peer).start)
    for o, k in enumerate(places):
        e_new[k, 0] = before[o][0]
        e_new[k, 1] = before[o][1]
        e_fade[k, 0] = before_d[o][0]
        e_fade[k, 1] = before_d[o][1]
    def local_pass(q, carry):
        total = resp[q]
        for t in range(QUARTER):
            tile = q * QUARTER + t
            for d in range(2):
                base = d * 256
                s_re, s_im = lead[tile, d, 0], lead[tile, d, 1]
                f_re, f_im = fade[tile, d, 0], fade[tile, d, 1]
                found = [None] * STEPS
                for j in range(STEPS) if d == 0 else range(STEPS - 1, -1, -1):
                    at = pl.ds(j * SUBS, SUBS)
                    a_re, a_im = dec[tile, at, base:base + 128], dec[tile, at, base + 128:base + 256]
                    n_re, n_im = times(a_re, a_im, s_re, s_im)
                    s_re = n_re + proj[tile, at, base:base + 128]
                    s_im = n_im + proj[tile, at, base + 128:base + 256]
                    f_re, f_im = times(a_re, a_im, f_re, f_im)
                    dec[tile, at, base:base + 128] = f_re
                    dec[tile, at, base + 128:base + 256] = f_im
                    found[j] = (s_re, s_im)
                    if j % 2 == (1 if d == 0 else 0):
                        first = j - j % 2
                        for part in range(2):
                            pair = jnp.concatenate([found[first][part], found[first + 1][part]], axis=0)
                            states[t, first * SUBS:(first + 2) * SUBS, base + part * 128:base + part * 128 + 128] = (
                                pair.astype(BF16)
                            )
            if t:
                total = total + jnp.dot(states[t - 1], cst[tile - 1], preferred_element_type=F32)
        resp[q] = total + jnp.dot(states[QUARTER - 1], cst[q * QUARTER + QUARTER - 1], preferred_element_type=F32)
        return carry

    lax.fori_loop(0, TILES // QUARTER, local_pass, 0)

    for k in range(1, LINES):
        peer, there = behind(k)
        pl.when(there)(u_in(k, peer).wait_recv)
    between = jnp.zeros((SUBS, 128), F32)
    for k in range(1, LINES):
        peer, there = behind(k)
        far_re, far_im = quarter_decay(between)
        x_far[k, 0] = far_re
        x_far[k, 1] = far_im
        between = between + jnp.where(there, t_line[peer], 0.0)

    gone = (zero, zero)
    for k in range(1, LINES):
        peer, there = behind(k)
        pl.when(there)(x_arr(k, peer).wait_recv)
        moved = times(x_far[k, 0], x_far[k, 1], x_in[peer, 0], x_in[peer, 1])
        gone = tuple(g + jnp.where(there, m, 0.0) for g, m in zip(gone, moved))
    for k in range(LINE):
        moved = times(e_fade[k, 0], e_fade[k, 1], *gone)
        e_new[k, 0] = e_new[k, 0] + moved[0]
        e_new[k, 1] = e_new[k, 1] + moved[1]
    for k in range(1, LINE):
        e_out(k).start()
    e_in[tp] = e_new[tp]
    for k in range(1, LINE):
        e_arr(k).wait_recv()

    def second_pass(q, carry):
        total = resp[q]
        for t in range(QUARTER):
            tile = q * QUARTER + t
            for d in range(2):
                base = d * 256
                e_re = jnp.broadcast_to(e_in[q * 2 + d, 0, t:t + 1, :], (16, 128))
                e_im = jnp.broadcast_to(e_in[q * 2 + d, 1, t:t + 1, :], (16, 128))
                for r in range(0, ROWS, 16):
                    f_re, f_im = dec[tile, r:r + 16, base:base + 128], dec[tile, r:r + 16, base + 128:base + 256]
                    m_re, m_im = times(f_re, f_im, e_re, e_im)
                    states[t, r:r + 16, base:base + 128] = m_re.astype(BF16)
                    states[t, r:r + 16, base + 128:base + 256] = m_im.astype(BF16)
            if t:
                total = total + jnp.dot(states[t - 1], cst[tile - 1], preferred_element_type=F32)
        resp[q] = total + jnp.dot(states[QUARTER - 1], cst[q * QUARTER + QUARTER - 1], preferred_element_type=F32)
        return carry

    lax.fori_loop(0, TILES // QUARTER, second_pass, 0)

    c_glu.wait()
    c_ow.wait()

    for k in range(1, LINE):
        t_out(k).wait_send()
        e_out(k).wait_send()
    for q in range(TILES // QUARTER):
        for d in range(2):
            pl.when(tp != q * 2 + d)(g_out(d, q).wait_send)
    for k in range(1, LINES):
        peer, there = ahead(k)
        pl.when(there)(u_out(k, peer).wait_send)
        pl.when(there)(x_out(k, peer).wait_send)


def output_unit(resp, glu_v, outw_v, gbias_v, ogain_v, out_ref):
    row_i = lax.broadcasted_iota(jnp.int32, (ROWS, ROWS), 0)
    col_i = lax.broadcasted_iota(jnp.int32, (ROWS, ROWS), 1)
    back = jnp.where(row_i == (col_i % SUBS) * STEPS + col_i // SUBS, 1.0, 0.0).astype(BF16)
    response = jnp.concatenate(
        [resp[m, :, 0:128] for m in range(4)] + [resp[m, :, 128:256] for m in range(4)], axis=1
    )
    active = jax.nn.gelu(response, approximate=True)
    active_low = active.astype(BF16)
    gates = []
    for n in range(4):
        at = slice(n * 256, (n + 1) * 256)
        gate = jnp.dot(active_low, glu_v[:, at], preferred_element_type=F32) + gbias_v[:, at]
        gates.append((active[:, at] * jax.nn.sigmoid(gate)).astype(BF16))
    gated = jnp.dot(back, jnp.concatenate(gates, axis=1), preferred_element_type=F32).astype(BF16)
    outs, square = [], None
    for n in range(8):
        at = slice(n * 256, (n + 1) * 256)
        piece = jnp.dot(gated, outw_v[:, at], preferred_element_type=F32)
        outs.append(piece)
        part = jnp.sum(piece * piece, axis=-1, keepdims=True)
        square = part if square is None else square + part
    scale = lax.rsqrt(square * (1.0 / 2048.0) + EPS)
    for n in range(8):
        at = slice(n * 256, (n + 1) * 256)
        out_ref[:, at] = (outs[n] * scale * ogain_v[:, at]).astype(BF16)


def local(
    tokens, elapsed, norm_gain, in_weight, state_input, state_output, forget_rate, decay_angle,
    skip_gain, glu_weight, glu_bias, out_weight, out_gain,
):
    args = (
        tokens, elapsed.reshape(1, -1), norm_gain.reshape(1, -1), in_weight, state_input.transpose(0, 1, 2, 4, 3),
        state_output, forget_rate, decay_angle, skip_gain.reshape(1, -1), glu_weight, out_weight,
    )
    vm = pltpu.VMEM
    scratch = [vm(a.shape, a.dtype) for a in args[:9]]
    scratch += [
        vm((ROWS, 2048), BF16),
        vm((ROWS, 1024), F32),
        vm((4, ROWS, 256), BF16),
        vm((4, 256, 512), BF16),
        vm((TILES, 512, 256), BF16),
        vm((TILES, ROWS, 512), F32),
        vm((TILES, ROWS, 512), F32),
        vm((2, 5, TILES, 128), F32),
        vm((2, ROWS, 128), BF16),
        vm((16, 128), F32),
        vm((QUARTER, 128, 512), BF16),
        vm((QUARTER, 128, 256), BF16),
        vm((QUARTER, ROWS, 256), F32),
        vm((QUARTER, ROWS, 512), BF16),
        vm((6, SUBS, 128), F32),
        vm((TILES, 2, 2, SUBS, 128), F32),
        vm((2, 4, 2, QUARTER, 128), F32),
        vm((TILES, 2, 2, SUBS, 128), F32),
        vm((TILES, 2, 2, SUBS, 128), F32),
        vm((LINE, SUBS, 128), F32),
        vm((LINES, SUBS, 128), F32),
        vm((LINE, 2, QUARTER, 128), F32),
        vm((LINES, 2, QUARTER, 128), F32),
        vm((LINES, 2, QUARTER, 128), F32),
        vm((LINE, 2, QUARTER, 128), F32),
        vm((LINE, 2, QUARTER, 128), F32),
        vm((LINE, 2, QUARTER, 128), F32),
        pltpu.SemaphoreType.DMA((16,)),
    ]
    for count in (LINE, LINES, LINE, LINES, LINE):
        scratch += [pltpu.SemaphoreType.DMA((count,)), pltpu.SemaphoreType.DMA((count,))]
    inner = pl.BlockSpec(memory_space=pltpu.VMEM)
    response, glu_held, out_held = pl.pallas_call(
        kernel,
        out_shape=(
            vm((4, ROWS, 256), F32),
            vm(glu_weight.shape, BF16),
            vm(out_weight.shape, BF16),
        ),
        in_specs=[pl.BlockSpec(memory_space=pltpu.HBM)] * len(args),
        out_specs=(inner, inner, inner),
        scratch_shapes=scratch,
        compiler_params=pltpu.CompilerParams(
            collective_id=0, has_side_effects=True, vmem_limit_bytes=50000000
        ),
        name="ssm_layer",
    )(*args)
    return pl.pallas_call(
        output_unit,
        out_shape=jax.ShapeDtypeStruct(tokens.shape, BF16),
        in_specs=[inner] * 5,
        out_specs=inner,
        compiler_params=pltpu.CompilerParams(vmem_limit_bytes=16000000),
        name="output_unit",
    )(response, glu_held, out_held, glu_bias.reshape(1, -1), out_gain.reshape(1, -1))


def solution(mesh):
    rows = P(("sp", "tp"), None)
    placed = (rows, P(("sp", "tp")), P(), P(), P(), P(), P(), P(), P(), P(), P(), P(), P())
    return jax.shard_map(local, mesh=mesh, in_specs=placed, out_specs=rows, check_vma=False)
```

```python
import functools
import math

import jax
import jax.numpy as jnp
from jax import lax
from jax.experimental import pallas as pl
from jax.experimental.pallas import tpu as pltpu
from jax.sharding import PartitionSpec as P

F32 = jnp.float32
BF16 = jnp.bfloat16
MESH = pl.DeviceIdType.MESH

ROWS = 128
TILES = 32
SUBS = 8
STEPS = 16
LINE = 8
LINES = 16
QUARTER = 8
EPS = 1e-06
LOG2E = 1.4426950408889634
SIN_C = (4.442883014678955, -7.308241367340088, 3.6062889099121094, -0.845763623714447, 0.10920575261116028)
COS_C = (1.4142135381698608, -6.9788641929626465, 5.73988151550293, -1.8882750272750854, 0.3322518765926361, -0.034502167254686356)
POINTS = [1.5 + 1.5 * math.cos((2 * i + 1) * math.pi / 32.0) for i in range(16)]
WEIGHTS = [1.0 / math.prod(p - o for o in POINTS if o != p) for p in POINTS]
INV_TURN = 1.0 / (2.0 * math.pi)
TURN_HI = math.floor(INV_TURN * 4096.0) / 4096.0
TURN_LO = INV_TURN - TURN_HI


def horner(x, coefficients):
    total = coefficients[-1]
    for c in coefficients[-2::-1]:
        total = total * x + c
    return total


def half_turn_parts(turns):
    part = turns - lax.round(turns, lax.RoundingMethod.TO_NEAREST_EVEN)
    square = part * part
    return part * horner(square, SIN_C), horner(square, COS_C)


def decay_parts(size, turns):
    sine, cosine = half_turn_parts(turns)
    lean = size * sine
    return size - lean * sine, lean * cosine


def in_parts(value, count):
    parts = []
    for _ in range(count):
        parts.append(value.astype(BF16))
        value = value - parts[-1].astype(F32)
    return parts


def times(a_re, a_im, b_re, b_im):
    return a_re * b_re - a_im * b_im, a_re * b_im + a_im * b_re


def kernel(
    tokens_h, elapsed_h, ngain_h, inw_h, sin_h, sout_h, rate_h, angle_h, skip_h, glu_h, outw_h,
    resp, glu_v, outw_v,
    tokens_v, elapsed_v, ngain_v, inw_v, sin_v, sout_v, rate_v, angle_v, skip_v,
    normed, acc, drv, bst, cst, proj, dec, tabs, by_token, at_node, cell_decay, cell_gain, gain, states, spans, loc, ssum, lead, fade,
    t_dev, t_line, g_in, x_in, x_far, e_new, e_fade, e_in,
    dma_sem, t_send, t_recv, u_send, u_recv, g_send, g_recv, x_send, x_recv, e_send, e_recv,
):
    sp = lax.axis_index("sp")
    tp = lax.axis_index("tp")
    yi, core = tp // 2, tp % 2
    way = core

    def line_peer(k):
        return {"sp": sp, "tp": k}

    def plane_peer(k):
        return {"sp": k, "tp": tp}

    def remote(src, dst, send_sem, recv_sem, peer):
        return pltpu.make_async_remote_copy(
            src_ref=src, dst_ref=dst, send_sem=send_sem, recv_sem=recv_sem, device_id=peer, device_id_type=MESH,
        )

    def ahead(step):
        k = jnp.where(way == 0, sp + step, sp - step)
        return lax.rem(k + LINES, LINES), jnp.logical_and(k >= 0, k < LINES)

    def behind(step):
        return ahead(-step)

    pairs = [
        (elapsed_h, elapsed_v), (tokens_h, tokens_v), (ngain_h, ngain_v), (rate_h, rate_v), (angle_h, angle_v),
        (sin_h, sin_v), (sout_h, sout_v), (skip_h, skip_v), (glu_h, glu_v), (outw_h, outw_v),
    ]
    copies = [pltpu.make_async_copy(a, b, dma_sem.at[k]) for k, (a, b) in enumerate(pairs)]
    c_el, c_tok, c_ng, c_rate, c_ang, c_sin, c_sout, c_skip, c_glu, c_ow = copies
    in_copies = [
        pltpu.make_async_copy(inw_h.at[pl.ds(k * 512, 512), :], inw_v.at[pl.ds(k * 512, 512), :], dma_sem.at[12 + k])
        for k in range(4)
    ]
    for c in (c_el, c_tok, c_ng, c_rate, c_ang):
        c.start()
    for c in in_copies:
        c.start()
    for c in (c_sin, c_sout, c_skip, c_glu, c_ow):
        c.start()

    barrier = pltpu.get_barrier_semaphore()
    for k in range(1, LINE):
        pl.semaphore_signal(barrier, inc=1, device_id=line_peer(lax.rem(tp + k, LINE)), device_id_type=MESH)
    for k in range(1, LINES):
        pl.semaphore_signal(barrier, inc=1, device_id=plane_peer(lax.rem(sp + k, LINES)), device_id_type=MESH)

    c_el.wait()
    steps = elapsed_v[...]
    whole = jnp.floor(steps)
    rest = steps - whole
    lane8 = lax.broadcasted_iota(jnp.int32, (SUBS, 128), 1)
    sub8 = lax.broadcasted_iota(jnp.int32, (SUBS, 128), 0)

    def picked(mask, row):
        total = jnp.sum(jnp.where(mask, jnp.broadcast_to(row, (SUBS, 128)), 0.0), axis=1, keepdims=True)
        return jnp.broadcast_to(total, (SUBS, 128))

    t_dev[tp] = jnp.where(sub8 == 0, picked(lane8 >= 0, whole), picked(lane8 >= 0, rest))
    gaps = [steps - p for p in POINTS]
    upto, after = [jnp.ones_like(steps)], [jnp.ones_like(steps)]
    for k in range(15):
        upto.append(upto[-1] * gaps[k])
        after.append(after[-1] * gaps[15 - k])
    basis = [upto[k] * after[15 - k] * WEIGHTS[k] for k in range(16)]
    scale = basis[0]
    for b in basis[1:]:
        scale = scale + b
    basis = jnp.concatenate(basis, axis=0) / jnp.broadcast_to(scale, (16, 128))
    b1, b2, b3 = in_parts(basis, 3)
    r1, r2 = in_parts(basis * jnp.sqrt(steps), 2)
    none16 = jnp.zeros((16, 128), BF16)
    token_rows = jnp.concatenate([b1, b1, b2, b2, b1, b3, none16, none16], axis=0)
    gain_rows = jnp.concatenate([r1, r1, r2] + [none16] * 5, axis=0)
    row_i = lax.broadcasted_iota(jnp.int32, (ROWS, ROWS), 0)
    col_i = lax.broadcasted_iota(jnp.int32, (ROWS, ROWS), 1)
    order = jnp.where(col_i == (row_i % SUBS) * STEPS + row_i // SUBS, 1.0, 0.0).astype(BF16)
    across = (((1,), (1,)), ((), ()))
    for k, rows in enumerate((token_rows, gain_rows)):
        by_token[k] = lax.dot_general(order, rows, across, preferred_element_type=F32).astype(BF16)
    node_i = lax.broadcasted_iota(jnp.int32, (16, 128), 0)
    nodes = jnp.full((16, 128), POINTS[0], F32)
    for k in range(1, 16):
        nodes = jnp.where(node_i == k, POINTS[k], nodes)
    at_node[...] = nodes
    none32 = jnp.zeros((32, 256), BF16)
    none80 = jnp.zeros((80, 256), BF16)
    for t in range(QUARTER):
        cell_decay[t, 96:128, :] = none32
    for t in range(QUARTER // 2):
        cell_gain[t, 48:128, :] = none80
    stretch = lane8 // STEPS
    for k, mask in enumerate((stretch == sub8, stretch > sub8, stretch < sub8)):
        spans[2 * k] = picked(mask, whole)
        spans[2 * k + 1] = picked(mask, rest)

    def t_out(k):
        peer = lax.rem(tp + k, LINE)
        return remote(t_dev.at[tp], t_dev.at[tp], t_send.at[k], t_recv.at[tp], line_peer(peer))

    def t_in(k):
        peer = lax.rem(tp + k, LINE)
        return remote(t_dev.at[peer], t_dev.at[peer], t_send.at[k], t_recv.at[peer], line_peer(peer))

    def u_out(k, peer):
        return remote(t_line.at[sp], t_line.at[sp], u_send.at[k], u_recv.at[sp], plane_peer(peer))

    def u_in(k, peer):
        return remote(t_line.at[peer], t_line.at[peer], u_send.at[k], u_recv.at[peer], plane_peer(peer))

    def x_out(k, peer):
        return remote(x_in.at[sp], x_in.at[sp], x_send.at[k], x_recv.at[sp], plane_peer(peer))

    def x_arr(k, peer):
        return remote(x_in.at[peer], x_in.at[peer], x_send.at[k], x_recv.at[peer], plane_peer(peer))

    def g_out(d, q):
        return remote(ssum.at[d, q], g_in.at[tp], g_send.at[q * 2 + d], g_recv.at[tp], line_peer(q * 2 + d))

    def g_arr(k):
        peer = lax.rem(tp + k, LINE)
        return remote(ssum.at[0, 0], g_in.at[peer], g_send.at[k], g_recv.at[peer], line_peer(peer))

    def e_out(k):
        peer = lax.rem(tp + k, LINE)
        return remote(e_new.at[peer], e_in.at[tp], e_send.at[k], e_recv.at[tp], line_peer(peer))

    c_rate.wait()
    c_ang.wait()
    for d in range(2):
        rate = jnp.concatenate([rate_v[d, 0:TILES, :], rate_v[d, TILES:, :]], axis=1)
        angle = jnp.concatenate([angle_v[d, 0:TILES, :], angle_v[d, TILES:, :]], axis=1)
        tabs[d, 0] = rate * (-LOG2E)
        tabs[d, 1] = rate * 2.0
        big = lax.round(angle * 1024.0, lax.RoundingMethod.TO_NEAREST_EVEN) * (1.0 / 1024.0)
        small = angle - big
        first = big * TURN_HI
        second = big * TURN_LO + (small * TURN_HI + small * TURN_LO)
        high = lax.round(first * 256.0, lax.RoundingMethod.TO_NEAREST_EVEN) * (1.0 / 256.0)
        low = (first - high) + second
        tabs[d, 2] = high
        tabs[d, 3] = low
        tabs[d, 4] = high + low

    def stretch_decay(rate2, high, low, both, t_whole, t_rest):
        size = jnp.exp2(rate2 * (t_whole + t_rest))
        turns = high * t_whole
        turns = turns - lax.round(turns, lax.RoundingMethod.TO_NEAREST_EVEN)
        return decay_parts(size, turns + low * t_whole + both * t_rest)

    def quarter_decay(t_tile):
        t_whole = jnp.broadcast_to(t_tile[0:1, :], (QUARTER, 128))
        t_rest = jnp.broadcast_to(t_tile[1:2, :], (QUARTER, 128))
        rows = pl.ds(pl.multiple_of(yi * QUARTER, QUARTER), QUARTER)
        return stretch_decay(*[tabs[way, k, rows, :] for k in (0, 2, 3, 4)], t_whole, t_rest)

    c_tok.wait()
    c_ng.wait()
    for r in range(4):
        x = tokens_v[pl.ds(r * 32, 32), :].astype(F32)
        scale = lax.rsqrt(jnp.mean(x * x, axis=-1, keepdims=True) + EPS)
        normed[pl.ds(r * 32, 32), :] = (x * scale * ngain_v[...]).astype(BF16)

    for k in range(4):
        in_copies[k].wait()
        part = jnp.dot(normed[:, k * 512:(k + 1) * 512], inw_v[k * 512:(k + 1) * 512, :], preferred_element_type=F32)
        acc[...] = part if k == 0 else acc[...] + part

    driven = jnp.dot(order, acc[...].astype(BF16), preferred_element_type=F32)
    c_skip.wait()
    for m in range(4):
        low_d, high_d = driven[:, m * 128:(m + 1) * 128], driven[:, 512 + m * 128:512 + (m + 1) * 128]
        resp[m, :, 0:128] = low_d * skip_v[:, m * 128:(m + 1) * 128]
        resp[m, :, 128:256] = high_d * skip_v[:, 512 + m * 128:512 + (m + 1) * 128]
        drv[m, :, 0:128] = low_d.astype(BF16)
        drv[m, :, 128:256] = high_d.astype(BF16)

    c_sin.wait()
    nothing = jnp.zeros((128, 64), BF16)
    for m in range(4):
        for d in range(2):
            for part in range(2):
                at = (d * 2 + part) * 128
                lower = sin_v[d, part, m * 8:(m + 1) * 8].reshape(128, 64)
                upper = sin_v[d, part, TILES + m * 8:TILES + (m + 1) * 8].reshape(128, 64)
                bst[m, 0:128, at:at + 128] = jnp.concatenate([lower, nothing], axis=1)
                bst[m, 128:256, at:at + 128] = jnp.concatenate([nothing, upper], axis=1)

    group_lane = (lax.broadcasted_iota(jnp.int32, (ROWS, 256), 1) // 16) % 8

    def first_pass(d, q):
        base = d * 256

        def values_at_nodes(t):
            row = pl.ds(q * QUARTER + t, 1)
            x = at_node[...]
            rate2, double, both = [jnp.broadcast_to(tabs[d, k, row, :], (16, 128)) for k in (0, 1, 4)]
            size = jnp.exp2(rate2 * x)
            y = double * x
            near = y * horner(y, (1.0, -0.5, 1.0 / 6.0, -1.0 / 24.0))
            gap = jnp.where(y < 0.03, near, 1.0 - size * size)
            for part, value in enumerate(decay_parts(size, both * x)):
                v1, v2, v3 = in_parts(value, 3)
                for k, v in enumerate((v1, v2, v1, v2, v3, v1)):
                    cell_decay[t, k * 16:(k + 1) * 16, part * 128:(part + 1) * 128] = v
            g1, g2 = in_parts(gap * lax.rsqrt(jnp.maximum(gap * x, 1e-37)), 2)
            at = slice(t % 2 * 128, t % 2 * 128 + 128)
            for k, v in enumerate((g1, g2, g1)):
                cell_gain[t // 2, k * 16:(k + 1) * 16, at] = v

        def products(t):
            gain[t // 2] = jnp.dot(by_token[1], cell_gain[t // 2], preferred_element_type=F32)
            for u in (t, t + 1):
                tile = q * QUARTER + u
                dec[tile, :, base:base + 256] = jnp.dot(by_token[0], cell_decay[u], preferred_element_type=F32)
                lhs = drv[q] * jnp.where(group_lane == u, 1.0, 0.0).astype(BF16)
                proj[tile, :, base:base + 256] = jnp.dot(
                    lhs, bst[q, :, base:base + 256], preferred_element_type=F32
                )

        def scan(t):
            tile = q * QUARTER + t
            s_re = s_im = None
            for j in range(STEPS) if d == 0 else range(STEPS - 1, -1, -1):
                at = pl.ds(j * SUBS, SUBS)
                damp = gain[t // 2, at, t % 2 * 128:t % 2 * 128 + 128]
                p_re = proj[tile, at, base:base + 128] * damp
                p_im = proj[tile, at, base + 128:base + 256] * damp
                proj[tile, at, base:base + 128] = p_re
                proj[tile, at, base + 128:base + 256] = p_im
                if s_re is None:
                    s_re, s_im = p_re, p_im
                else:
                    a_re, a_im = dec[tile, at, base:base + 128], dec[tile, at, base + 128:base + 256]
                    n_re, n_im = times(a_re, a_im, s_re, s_im)
                    s_re, s_im = n_re + p_re, n_im + p_im
            loc[tile, d, 0] = s_re
            loc[tile, d, 1] = s_im
            k = 2 if d == 0 else 4
            rate2, high, low, both = [
                jnp.broadcast_to(tabs[d, i, pl.ds(tile, 1), :], (SUBS, 128)) for i in (0, 2, 3, 4)
            ]
            w_re, w_im = stretch_decay(rate2, high, low, both, spans[k], spans[k + 1])
            m_re, m_im = times(w_re, w_im, s_re, s_im)
            ssum[d, q, 0, t:t + 1, :] = jnp.sum(m_re, axis=0, keepdims=True)
            ssum[d, q, 1, t:t + 1, :] = jnp.sum(m_im, axis=0, keepdims=True)

        for t in (0, 1):
            values_at_nodes(t)
        products(0)
        for t in (2, 3):
            values_at_nodes(t)
        for t in range(0, QUARTER, 2):
            if t + 2 < QUARTER:
                products(t + 2)
            for u in (t, t + 1):
                if u + 4 < QUARTER:
                    values_at_nodes(u + 4)
                scan(u)

    def backward_quarter(q, carry):
        @pl.when(q == 2)
        def _():
            pl.semaphore_wait(barrier, LINE - 1 + LINES - 1)
            for k in range(1, LINE):
                t_out(k).start()
            pl.when(tp != 1)(g_out(1, 0).start)

        pl.when(jnp.logical_and(q >= 2, tp != q * 2 - 1))(g_out(1, q - 1).start)

        first_pass(1, q)
        return carry

    def forward_quarter(q, carry):
        first_pass(0, q)
        pl.when(tp != q * 2)(g_out(0, q).start)
        return carry

    lax.fori_loop(0, TILES // QUARTER, backward_quarter, 0)
    pl.when(tp != LINE - 1)(g_out(1, TILES // QUARTER - 1).start)
    lax.fori_loop(0, TILES // QUARTER, forward_quarter, 0)

    def lead_in(tile, carry):
        for d in range(2):
            rate2, _, high, low, both = [
                jnp.broadcast_to(tabs[d, k, pl.ds(tile, 1), :], (SUBS, 128)) for k in range(5)
            ]
            g_re, g_im = stretch_decay(rate2, high, low, both, spans[0], spans[1])
            x_re, x_im = loc[tile, d, 0], loc[tile, d, 1]
            for hop in (1, 2, 4):
                turn = hop if d == 0 else SUBS - hop
                inside = sub8 >= hop if d == 0 else sub8 < SUBS - hop
                q_re, q_im, h_re, h_im = [pltpu.roll(v, turn, 0) for v in (x_re, x_im, g_re, g_im)]
                m_re, m_im = times(g_re, g_im, q_re, q_im)
                n_re, n_im = times(g_re, g_im, h_re, h_im)
                x_re, x_im = jnp.where(inside, x_re + m_re, x_re), jnp.where(inside, x_im + m_im, x_im)
                g_re, g_im = jnp.where(inside, n_re, g_re), jnp.where(inside, n_im, g_im)
            turn = 1 if d == 0 else SUBS - 1
            inside = sub8 >= 1 if d == 0 else sub8 < SUBS - 1
            x_re, x_im, g_re, g_im = [
                jnp.where(inside, pltpu.roll(v, turn, 0), blank_value)
                for v, blank_value in ((x_re, 0.0), (x_im, 0.0), (g_re, 1.0), (g_im, 0.0))
            ]
            lead[tile, d, 0] = x_re
            lead[tile, d, 1] = x_im
            fade[tile, d, 0] = g_re
            fade[tile, d, 1] = g_im
        return carry

    lane_group = lax.broadcasted_iota(jnp.int32, (64, 128), 1) // 16
    blank = jnp.zeros((64, 128), BF16)

    def spread(m, carry):
        for d in range(2):
            for part in range(2):
                sign = 1.0 if part == 0 else -1.0
                at = (d * 2 + part) * 128
                lower = (sout_v[d, part, pl.ds(m * 8, 8)].reshape(128, 64) * sign).T
                upper = (sout_v[d, part, pl.ds(TILES + m * 8, 8)].reshape(128, 64) * sign).T
                for i in range(8):
                    tile = m * 8 + i
                    cst[tile, at:at + 64, 0:128] = jnp.where(lane_group == i, lower, 0.0).astype(BF16)
                    cst[tile, at:at + 64, 128:256] = blank
                    cst[tile, at + 64:at + 128, 0:128] = blank
                    cst[tile, at + 64:at + 128, 128:256] = jnp.where(lane_group == i, upper, 0.0).astype(BF16)
        return carry


    def own_work():
        lax.fori_loop(0, TILES, lead_in, 0)
        lax.fori_loop(0, 4, spread, 0)

    def pass_on_elapsed():
        for k in range(1, LINE):
            t_in(k).wait_recv()
        total = t_dev[0]
        for k in range(1, LINE):
            total = total + t_dev[k]
        t_line[sp] = total
        for k in range(1, LINES):
            peer, there = ahead(k)
            pl.when(there)(u_out(k, peer).start)

    c_sout.wait()

    @pl.when(core == 0)
    def _():
        own_work()

    pass_on_elapsed()

    g_in[tp] = ssum[way, yi]
    places = [jnp.where(way == 0, o, LINE - 1 - o) for o in range(LINE)]
    gains = [quarter_decay(t_dev[k]) for k in places]
    for k in range(1, LINE):
        g_arr(k).wait_recv()
    zero, one = jnp.zeros((QUARTER, 128), F32), jnp.ones((QUARTER, 128), F32)
    run, run_d, before, before_d = (zero, zero), (one, zero), [], []
    for o, k in enumerate(places):
        before.append(run)
        before_d.append(run_d)
        moved = times(*gains[o], *run)
        run = (moved[0] + g_in[k, 0], moved[1] + g_in[k, 1])
        run_d = times(*gains[o], *run_d)
    x_in[sp, 0] = run[0]
    x_in[sp, 1] = run[1]
    for k in range(1, LINES):
        peer, there = ahead(k)
        pl.when(there)(x_out(k, peer).start)
    for o, k in enumerate(places):
        e_new[k, 0] = before[o][0]
        e_new[k, 1] = before[o][1]
        e_fade[k, 0] = before_d[o][0]
        e_fade[k, 1] = before_d[o][1]
    @pl.when(core == 1)
    def _():
        own_work()

    def local_pass(q, carry):
        total = resp[q]
        for t in range(QUARTER):
            tile = q * QUARTER + t
            for d in range(2):
                base = d * 256
                s_re, s_im = lead[tile, d, 0], lead[tile, d, 1]
                f_re, f_im = fade[tile, d, 0], fade[tile, d, 1]
                found = [None] * STEPS
                for j in range(STEPS) if d == 0 else range(STEPS - 1, -1, -1):
                    at = pl.ds(j * SUBS, SUBS)
                    a_re, a_im = dec[tile, at, base:base + 128], dec[tile, at, base + 128:base + 256]
                    n_re, n_im = times(a_re, a_im, s_re, s_im)
                    s_re = n_re + proj[tile, at, base:base + 128]
                    s_im = n_im + proj[tile, at, base + 128:base + 256]
                    f_re, f_im = times(a_re, a_im, f_re, f_im)
                    dec[tile, at, base:base + 128] = f_re
                    dec[tile, at, base + 128:base + 256] = f_im
                    found[j] = (s_re, s_im)
                    if j % 2 == (1 if d == 0 else 0):
                        first = j - j % 2
                        for part in range(2):
                            pair = jnp.concatenate([found[first][part], found[first + 1][part]], axis=0)
                            states[t, first * SUBS:(first + 2) * SUBS, base + part * 128:base + part * 128 + 128] = (
                                pair.astype(BF16)
                            )
            if t:
                total = total + jnp.dot(states[t - 1], cst[tile - 1], preferred_element_type=F32)
        resp[q] = total + jnp.dot(states[QUARTER - 1], cst[q * QUARTER + QUARTER - 1], preferred_element_type=F32)
        return carry

    lax.fori_loop(0, 2, local_pass, 0)

    for k in range(1, LINES):
        peer, there = behind(k)
        pl.when(there)(u_in(k, peer).wait_recv)
    between = jnp.zeros((SUBS, 128), F32)
    for k in range(1, LINES):
        peer, there = behind(k)
        far_re, far_im = quarter_decay(between)
        x_far[k, 0] = far_re
        x_far[k, 1] = far_im
        between = between + jnp.where(there, t_line[peer], 0.0)

    gone = (zero, zero)
    for k in range(1, LINES):
        peer, there = behind(k)
        pl.when(there)(x_arr(k, peer).wait_recv)
        moved = times(x_far[k, 0], x_far[k, 1], x_in[peer, 0], x_in[peer, 1])
        gone = tuple(g + jnp.where(there, m, 0.0) for g, m in zip(gone, moved))
    for k in range(LINE):
        moved = times(e_fade[k, 0], e_fade[k, 1], *gone)
        e_new[k, 0] = e_new[k, 0] + moved[0]
        e_new[k, 1] = e_new[k, 1] + moved[1]
    for k in range(1, LINE):
        e_out(k).start()
    e_in[tp] = e_new[tp]
    def second_pass(d):
        base = d * 256
        for chip in range(4):
            k = chip * 2 + d
            pl.when(tp != k)(remote(e_new.at[k], e_in.at[k], e_send.at[0], e_recv.at[k], line_peer(k)).wait_recv)

        def quarter(q, carry):
            total = resp[q]
            for t in range(QUARTER):
                tile = q * QUARTER + t
                e_re = jnp.broadcast_to(e_in[q * 2 + d, 0, t:t + 1, :], (16, 128))
                e_im = jnp.broadcast_to(e_in[q * 2 + d, 1, t:t + 1, :], (16, 128))
                for r in range(0, ROWS, 16):
                    f_re, f_im = dec[tile, r:r + 16, base:base + 128], dec[tile, r:r + 16, base + 128:base + 256]
                    m_re, m_im = times(f_re, f_im, e_re, e_im)
                    states[t, r:r + 16, base:base + 128] = m_re.astype(BF16)
                    states[t, r:r + 16, base + 128:base + 256] = m_im.astype(BF16)
                total = total + jnp.dot(
                    states[t, :, base:base + 256], cst[tile, base:base + 256, :], preferred_element_type=F32
                )
            resp[q] = total
            return carry

        for q in range(TILES // QUARTER):
            quarter(q, 0)

    lax.fori_loop(2, 4, local_pass, 0)
    second_pass(0)
    second_pass(1)

    c_glu.wait()
    c_ow.wait()

    for k in range(1, LINE):
        t_out(k).wait_send()
        e_out(k).wait_send()
    for q in range(TILES // QUARTER):
        for d in range(2):
            pl.when(tp != q * 2 + d)(g_out(d, q).wait_send)
    for k in range(1, LINES):
        peer, there = ahead(k)
        pl.when(there)(u_out(k, peer).wait_send)
        pl.when(there)(x_out(k, peer).wait_send)


def output_unit(resp, glu_v, outw_v, gbias_v, ogain_v, out_ref):
    row_i = lax.broadcasted_iota(jnp.int32, (ROWS, ROWS), 0)
    col_i = lax.broadcasted_iota(jnp.int32, (ROWS, ROWS), 1)
    back = jnp.where(row_i == (col_i % SUBS) * STEPS + col_i // SUBS, 1.0, 0.0).astype(BF16)
    response = jnp.concatenate(
        [resp[m, :, 0:128] for m in range(4)] + [resp[m, :, 128:256] for m in range(4)], axis=1
    )
    active = jax.nn.gelu(response, approximate=True)
    active_low = active.astype(BF16)
    gates = []
    for n in range(4):
        at = slice(n * 256, (n + 1) * 256)
        gate = jnp.dot(active_low, glu_v[:, at], preferred_element_type=F32) + gbias_v[:, at]
        gates.append((active[:, at] * jax.nn.sigmoid(gate)).astype(BF16))
    gated = jnp.dot(back, jnp.concatenate(gates, axis=1), preferred_element_type=F32).astype(BF16)
    outs, square = [], None
    for n in range(8):
        at = slice(n * 256, (n + 1) * 256)
        piece = jnp.dot(gated, outw_v[:, at], preferred_element_type=F32)
        outs.append(piece)
        part = jnp.sum(piece * piece, axis=-1, keepdims=True)
        square = part if square is None else square + part
    scale = lax.rsqrt(square * (1.0 / 2048.0) + EPS)
    for n in range(8):
        at = slice(n * 256, (n + 1) * 256)
        out_ref[:, at] = (outs[n] * scale * ogain_v[:, at]).astype(BF16)


def local(
    tokens, elapsed, norm_gain, in_weight, state_input, state_output, forget_rate, decay_angle,
    skip_gain, glu_weight, glu_bias, out_weight, out_gain,
):
    args = (
        tokens, elapsed.reshape(1, -1), norm_gain.reshape(1, -1), in_weight, state_input.transpose(0, 1, 2, 4, 3),
        state_output, forget_rate, decay_angle, skip_gain.reshape(1, -1), glu_weight, out_weight,
    )
    vm = pltpu.VMEM
    scratch = [vm(a.shape, a.dtype) for a in args[:9]]
    scratch += [
        vm((ROWS, 2048), BF16),
        vm((ROWS, 1024), F32),
        vm((4, ROWS, 256), BF16),
        vm((4, 256, 512), BF16),
        vm((TILES, 512, 256), BF16),
        vm((TILES, ROWS, 512), F32),
        vm((TILES, ROWS, 512), F32),
        vm((2, 5, TILES, 128), F32),
        vm((2, ROWS, 128), BF16),
        vm((16, 128), F32),
        vm((QUARTER, 128, 256), BF16),
        vm((QUARTER // 2, 128, 256), BF16),
        vm((QUARTER // 2, ROWS, 256), F32),
        vm((QUARTER, ROWS, 512), BF16),
        vm((6, SUBS, 128), F32),
        vm((TILES, 2, 2, SUBS, 128), F32),
        vm((2, 4, 2, QUARTER, 128), F32),
        vm((TILES, 2, 2, SUBS, 128), F32),
        vm((TILES, 2, 2, SUBS, 128), F32),
        vm((LINE, SUBS, 128), F32),
        vm((LINES, SUBS, 128), F32),
        vm((LINE, 2, QUARTER, 128), F32),
        vm((LINES, 2, QUARTER, 128), F32),
        vm((LINES, 2, QUARTER, 128), F32),
        vm((LINE, 2, QUARTER, 128), F32),
        vm((LINE, 2, QUARTER, 128), F32),
        vm((LINE, 2, QUARTER, 128), F32),
        pltpu.SemaphoreType.DMA((16,)),
    ]
    for count in (LINE, LINES, LINE, LINES, LINE):
        scratch += [pltpu.SemaphoreType.DMA((count,)), pltpu.SemaphoreType.DMA((count,))]
    inner = pl.BlockSpec(memory_space=pltpu.VMEM)
    response, glu_held, out_held = pl.pallas_call(
        kernel,
        out_shape=(
            vm((4, ROWS, 256), F32),
            vm(glu_weight.shape, BF16),
            vm(out_weight.shape, BF16),
        ),
        in_specs=[pl.BlockSpec(memory_space=pltpu.HBM)] * len(args),
        out_specs=(inner, inner, inner),
        scratch_shapes=scratch,
        compiler_params=pltpu.CompilerParams(
            collective_id=0, has_side_effects=True, vmem_limit_bytes=50000000
        ),
        name="ssm_layer",
    )(*args)
    return pl.pallas_call(
        output_unit,
        out_shape=jax.ShapeDtypeStruct(tokens.shape, BF16),
        in_specs=[inner] * 5,
        out_specs=inner,
        compiler_params=pltpu.CompilerParams(vmem_limit_bytes=16000000),
        name="output_unit",
    )(response, glu_held, out_held, glu_bias.reshape(1, -1), out_gain.reshape(1, -1))


def solution(mesh):
    rows = P(("sp", "tp"), None)
    placed = (rows, P(("sp", "tp")), P(), P(), P(), P(), P(), P(), P(), P(), P(), P(), P())
    return jax.shard_map(local, mesh=mesh, in_specs=placed, out_specs=rows, check_vma=False)
```

```python
import functools
import math

import jax
import jax.numpy as jnp
from jax import lax
from jax.experimental import pallas as pl
from jax.experimental.pallas import tpu as pltpu
from jax.sharding import PartitionSpec as P

F32 = jnp.float32
BF16 = jnp.bfloat16
MESH = pl.DeviceIdType.MESH

ROWS = 128
TILES = 32
SUBS = 8
STEPS = 16
LINE = 8
LINES = 16
QUARTER = 8
EPS = 1e-06
LOG2E = 1.4426950408889634
SIN_C = (4.442883014678955, -7.308241367340088, 3.6062889099121094, -0.845763623714447, 0.10920575261116028)
COS_C = (1.4142135381698608, -6.9788641929626465, 5.73988151550293, -1.8882750272750854, 0.3322518765926361, -0.034502167254686356)
POINTS = [1.5 + 1.5 * math.cos((2 * i + 1) * math.pi / 32.0) for i in range(16)]
WEIGHTS = [1.0 / math.prod(p - o for o in POINTS if o != p) for p in POINTS]
INV_TURN = 1.0 / (2.0 * math.pi)
TURN_HI = math.floor(INV_TURN * 4096.0) / 4096.0
TURN_LO = INV_TURN - TURN_HI


def horner(x, coefficients):
    total = coefficients[-1]
    for c in coefficients[-2::-1]:
        total = total * x + c
    return total


def half_turn_parts(turns):
    part = turns - lax.round(turns, lax.RoundingMethod.TO_NEAREST_EVEN)
    square = part * part
    return part * horner(square, SIN_C), horner(square, COS_C)


def decay_parts(size, turns):
    sine, cosine = half_turn_parts(turns)
    lean = size * sine
    return size - lean * sine, lean * cosine


def in_parts(value, count):
    parts = []
    for _ in range(count):
        parts.append(value.astype(BF16))
        value = value - parts[-1].astype(F32)
    return parts


def times(a_re, a_im, b_re, b_im):
    return a_re * b_re - a_im * b_im, a_re * b_im + a_im * b_re


def kernel(
    tokens_h, elapsed_h, ngain_h, inw_h, sin_h, sout_h, rate_h, angle_h, skip_h, glu_h, outw_h,
    resp, glu_v, outw_v,
    tokens_v, elapsed_v, ngain_v, inw_v, sin_v, sout_v, rate_v, angle_v, skip_v,
    normed, acc, drv, bst, cst, proj, dec, tabs, by_token, at_node, cell_decay, cell_gain, gain, states, spans, loc, ssum, lead, fade,
    t_dev, t_line, g_in, x_in, x_far, e_new, e_fade, e_in,
    dma_sem, t_send, t_recv, u_send, u_recv, g_send, g_recv, x_send, x_recv, e_send, e_recv,
):
    sp = lax.axis_index("sp")
    tp = lax.axis_index("tp")
    yi, core = tp // 2, tp % 2
    way = core

    def line_peer(k):
        return {"sp": sp, "tp": k}

    def plane_peer(k):
        return {"sp": k, "tp": tp}

    def remote(src, dst, send_sem, recv_sem, peer):
        return pltpu.make_async_remote_copy(
            src_ref=src, dst_ref=dst, send_sem=send_sem, recv_sem=recv_sem, device_id=peer, device_id_type=MESH,
        )

    def ahead(step):
        k = jnp.where(way == 0, sp + step, sp - step)
        return lax.rem(k + LINES, LINES), jnp.logical_and(k >= 0, k < LINES)

    def behind(step):
        return ahead(-step)

    pairs = [
        (elapsed_h, elapsed_v), (tokens_h, tokens_v), (ngain_h, ngain_v), (rate_h, rate_v), (angle_h, angle_v),
        (sin_h, sin_v), (sout_h, sout_v), (skip_h, skip_v), (glu_h, glu_v), (outw_h, outw_v),
    ]
    copies = [pltpu.make_async_copy(a, b, dma_sem.at[k]) for k, (a, b) in enumerate(pairs)]
    c_el, c_tok, c_ng, c_rate, c_ang, c_sin, c_sout, c_skip, c_glu, c_ow = copies
    in_copies = [
        pltpu.make_async_copy(inw_h.at[pl.ds(k * 512, 512), :], inw_v.at[pl.ds(k * 512, 512), :], dma_sem.at[11 + k])
        for k in range(4)
    ]
    for c in (c_el, c_tok, c_ng, c_rate, c_ang):
        c.start()
    for c in in_copies:
        c.start()
    for c in (c_sin, c_sout, c_skip, c_glu, c_ow):
        c.start()

    barrier = pltpu.get_barrier_semaphore()
    for k in range(1, LINE):
        pl.semaphore_signal(barrier, inc=1, device_id=line_peer(lax.rem(tp + k, LINE)), device_id_type=MESH)
    for k in range(1, LINES):
        pl.semaphore_signal(barrier, inc=1, device_id=plane_peer(lax.rem(sp + k, LINES)), device_id_type=MESH)

    c_el.wait()
    steps = elapsed_v[...]
    whole = jnp.floor(steps)
    rest = steps - whole
    lane8 = lax.broadcasted_iota(jnp.int32, (SUBS, 128), 1)
    sub8 = lax.broadcasted_iota(jnp.int32, (SUBS, 128), 0)

    def picked(mask, row):
        total = jnp.sum(jnp.where(mask, jnp.broadcast_to(row, (SUBS, 128)), 0.0), axis=1, keepdims=True)
        return jnp.broadcast_to(total, (SUBS, 128))

    t_dev[tp] = jnp.where(sub8 == 0, picked(lane8 >= 0, whole), picked(lane8 >= 0, rest))
    gaps = [steps - p for p in POINTS]
    upto, after = [jnp.ones_like(steps)], [jnp.ones_like(steps)]
    for k in range(15):
        upto.append(upto[-1] * gaps[k])
        after.append(after[-1] * gaps[15 - k])
    basis = [upto[k] * after[15 - k] * WEIGHTS[k] for k in range(16)]
    scale = basis[0]
    for b in basis[1:]:
        scale = scale + b
    basis = jnp.concatenate(basis, axis=0) / jnp.broadcast_to(scale, (16, 128))
    b1, b2, b3 = in_parts(basis, 3)
    r1, r2 = in_parts(basis * jnp.sqrt(steps), 2)
    none16 = jnp.zeros((16, 128), BF16)
    token_rows = jnp.concatenate([b1, b1, b2, b2, b1, b3, none16, none16], axis=0)
    gain_rows = jnp.concatenate([r1, r1, r2] + [none16] * 5, axis=0)
    row_i = lax.broadcasted_iota(jnp.int32, (ROWS, ROWS), 0)
    col_i = lax.broadcasted_iota(jnp.int32, (ROWS, ROWS), 1)
    order = jnp.where(col_i == (row_i % SUBS) * STEPS + row_i // SUBS, 1.0, 0.0).astype(BF16)
    across = (((1,), (1,)), ((), ()))
    for k, rows in enumerate((token_rows, gain_rows)):
        by_token[k] = lax.dot_general(order, rows, across, preferred_element_type=F32).astype(BF16)
    node_i = lax.broadcasted_iota(jnp.int32, (16, 128), 0)
    nodes = jnp.full((16, 128), POINTS[0], F32)
    for k in range(1, 16):
        nodes = jnp.where(node_i == k, POINTS[k], nodes)
    at_node[...] = nodes
    none32 = jnp.zeros((32, 256), BF16)
    none80 = jnp.zeros((80, 256), BF16)
    for t in range(QUARTER):
        cell_decay[t, 96:128, :] = none32
    for t in range(QUARTER // 2):
        cell_gain[t, 48:128, :] = none80
    stretch = lane8 // STEPS
    for k, mask in enumerate((stretch == sub8, stretch > sub8, stretch < sub8)):
        spans[2 * k] = picked(mask, whole)
        spans[2 * k + 1] = picked(mask, rest)

    def t_out(k):
        return remote(t_dev.at[tp], t_dev.at[tp], t_send.at[0], t_recv.at[0], line_peer(lax.rem(tp + k, LINE)))

    def u_out(peer):
        return remote(t_line.at[sp], t_line.at[sp], u_send.at[0], u_recv.at[0], plane_peer(peer))

    def x_out(peer):
        return remote(x_in.at[sp], x_in.at[sp], x_send.at[0], x_recv.at[0], plane_peer(peer))

    def g_out(d, q):
        return remote(ssum.at[d, q], g_in.at[tp], g_send.at[0], g_recv.at[0], line_peer(q * 2 + d))

    def e_out(k):
        peer = lax.rem(tp + k, LINE)
        return remote(e_new.at[peer], e_in.at[tp], e_send.at[0], e_recv.at[core], line_peer(peer))

    def blocks(buf, n, send_sem, recv_sem):
        part = buf.at[pl.ds(0, n)]
        return remote(part, part, send_sem, recv_sem, line_peer(lax.rem(tp + 1, LINE)))

    lines_behind = jnp.where(way == 0, sp, LINES - 1 - sp)
    lines_ahead = LINES - 1 - lines_behind

    def lines_in(buf, send_sem, recv_sem):
        for n in range(1, LINES):
            pl.when(lines_behind == n)(blocks(buf, n, send_sem, recv_sem).wait_recv)

    def lines_out(buf, send_sem, recv_sem):
        for n in range(1, LINES):
            pl.when(lines_ahead == n)(blocks(buf, n, send_sem, recv_sem).wait_send)

    c_rate.wait()
    c_ang.wait()
    for d in range(2):
        rate = jnp.concatenate([rate_v[d, 0:TILES, :], rate_v[d, TILES:, :]], axis=1)
        angle = jnp.concatenate([angle_v[d, 0:TILES, :], angle_v[d, TILES:, :]], axis=1)
        tabs[d, 0] = rate * (-LOG2E)
        tabs[d, 1] = rate * 2.0
        big = lax.round(angle * 1024.0, lax.RoundingMethod.TO_NEAREST_EVEN) * (1.0 / 1024.0)
        small = angle - big
        first = big * TURN_HI
        second = big * TURN_LO + (small * TURN_HI + small * TURN_LO)
        high = lax.round(first * 256.0, lax.RoundingMethod.TO_NEAREST_EVEN) * (1.0 / 256.0)
        low = (first - high) + second
        tabs[d, 2] = high
        tabs[d, 3] = low
        tabs[d, 4] = high + low

    def stretch_decay(rate2, high, low, both, t_whole, t_rest):
        size = jnp.exp2(rate2 * (t_whole + t_rest))
        turns = high * t_whole
        turns = turns - lax.round(turns, lax.RoundingMethod.TO_NEAREST_EVEN)
        return decay_parts(size, turns + low * t_whole + both * t_rest)

    def quarter_decay(t_tile):
        t_whole = jnp.broadcast_to(t_tile[0:1, :], (QUARTER, 128))
        t_rest = jnp.broadcast_to(t_tile[1:2, :], (QUARTER, 128))
        rows = pl.ds(pl.multiple_of(yi * QUARTER, QUARTER), QUARTER)
        return stretch_decay(*[tabs[way, k, rows, :] for k in (0, 2, 3, 4)], t_whole, t_rest)

    c_tok.wait()
    c_ng.wait()
    for r in range(4):
        x = tokens_v[pl.ds(r * 32, 32), :].astype(F32)
        scale = lax.rsqrt(jnp.mean(x * x, axis=-1, keepdims=True) + EPS)
        normed[pl.ds(r * 32, 32), :] = (x * scale * ngain_v[...]).astype(BF16)

    for k in range(4):
        in_copies[k].wait()
        part = jnp.dot(normed[:, k * 512:(k + 1) * 512], inw_v[k * 512:(k + 1) * 512, :], preferred_element_type=F32)
        acc[...] = part if k == 0 else acc[...] + part

    driven = jnp.dot(order, acc[...].astype(BF16), preferred_element_type=F32)
    c_skip.wait()
    for m in range(4):
        low_d, high_d = driven[:, m * 128:(m + 1) * 128], driven[:, 512 + m * 128:512 + (m + 1) * 128]
        resp[m, :, 0:128] = low_d * skip_v[:, m * 128:(m + 1) * 128]
        resp[m, :, 128:256] = high_d * skip_v[:, 512 + m * 128:512 + (m + 1) * 128]
        drv[m, :, 0:128] = low_d.astype(BF16)
        drv[m, :, 128:256] = high_d.astype(BF16)

    c_sin.wait()
    nothing = jnp.zeros((128, 64), BF16)
    for m in range(4):
        for d in range(2):
            for part in range(2):
                at = (d * 2 + part) * 128
                lower = sin_v[d, part, m * 8:(m + 1) * 8].reshape(128, 64)
                upper = sin_v[d, part, TILES + m * 8:TILES + (m + 1) * 8].reshape(128, 64)
                bst[m, 0:128, at:at + 128] = jnp.concatenate([lower, nothing], axis=1)
                bst[m, 128:256, at:at + 128] = jnp.concatenate([nothing, upper], axis=1)

    group_lane = (lax.broadcasted_iota(jnp.int32, (ROWS, 256), 1) // 16) % 8

    def first_pass(d, q):
        base = d * 256

        def values_at_nodes(t):
            row = pl.ds(q * QUARTER + t, 1)
            x = at_node[...]
            rate2, double, both = [jnp.broadcast_to(tabs[d, k, row, :], (16, 128)) for k in (0, 1, 4)]
            size = jnp.exp2(rate2 * x)
            y = double * x
            near = y * horner(y, (1.0, -0.5, 1.0 / 6.0, -1.0 / 24.0))
            gap = jnp.where(y < 0.03, near, 1.0 - size * size)
            for part, value in enumerate(decay_parts(size, both * x)):
                v1, v2, v3 = in_parts(value, 3)
                for k, v in enumerate((v1, v2, v1, v2, v3, v1)):
                    cell_decay[t, k * 16:(k + 1) * 16, part * 128:(part + 1) * 128] = v
            g1, g2 = in_parts(gap * lax.rsqrt(jnp.maximum(gap * x, 1e-37)), 2)
            at = slice(t % 2 * 128, t % 2 * 128 + 128)
            for k, v in enumerate((g1, g2, g1)):
                cell_gain[t // 2, k * 16:(k + 1) * 16, at] = v

        def products(t):
            gain[t // 2] = jnp.dot(by_token[1], cell_gain[t // 2], preferred_element_type=F32)
            for u in (t, t + 1):
                tile = q * QUARTER + u
                dec[tile, :, base:base + 256] = jnp.dot(by_token[0], cell_decay[u], preferred_element_type=F32)
                lhs = drv[q] * jnp.where(group_lane == u, 1.0, 0.0).astype(BF16)
                proj[tile, :, base:base + 256] = jnp.dot(
                    lhs, bst[q, :, base:base + 256], preferred_element_type=F32
                )

        def scan(t):
            tile = q * QUARTER + t
            s_re = s_im = None
            for j in range(STEPS) if d == 0 else range(STEPS - 1, -1, -1):
                at = pl.ds(j * SUBS, SUBS)
                damp = gain[t // 2, at, t % 2 * 128:t % 2 * 128 + 128]
                p_re = proj[tile, at, base:base + 128] * damp
                p_im = proj[tile, at, base + 128:base + 256] * damp
                proj[tile, at, base:base + 128] = p_re
                proj[tile, at, base + 128:base + 256] = p_im
                if s_re is None:
                    s_re, s_im = p_re, p_im
                else:
                    a_re, a_im = dec[tile, at, base:base + 128], dec[tile, at, base + 128:base + 256]
                    n_re, n_im = times(a_re, a_im, s_re, s_im)
                    s_re, s_im = n_re + p_re, n_im + p_im
            loc[tile, d, 0] = s_re
            loc[tile, d, 1] = s_im
            k = 2 if d == 0 else 4
            rate2, high, low, both = [
                jnp.broadcast_to(tabs[d, i, pl.ds(tile, 1), :], (SUBS, 128)) for i in (0, 2, 3, 4)
            ]
            w_re, w_im = stretch_decay(rate2, high, low, both, spans[k], spans[k + 1])
            m_re, m_im = times(w_re, w_im, s_re, s_im)
            ssum[d, q, 0, t:t + 1, :] = jnp.sum(m_re, axis=0, keepdims=True)
            ssum[d, q, 1, t:t + 1, :] = jnp.sum(m_im, axis=0, keepdims=True)

        for t in (0, 1):
            values_at_nodes(t)
        products(0)
        for t in (2, 3):
            values_at_nodes(t)
        for t in range(0, QUARTER, 2):
            if t + 2 < QUARTER:
                products(t + 2)
            for u in (t, t + 1):
                if u + 4 < QUARTER:
                    values_at_nodes(u + 4)
                scan(u)

    def backward_quarter(q, carry):
        @pl.when(q == 2)
        def _():
            pl.semaphore_wait(barrier, LINE - 1 + LINES - 1)
            for k in range(1, LINE):
                t_out(k).start()
            pl.when(tp != 1)(g_out(1, 0).start)

        pl.when(jnp.logical_and(q >= 2, tp != q * 2 - 1))(g_out(1, q - 1).start)

        first_pass(1, q)
        return carry

    def forward_quarter(q, carry):
        first_pass(0, q)
        pl.when(tp != q * 2)(g_out(0, q).start)
        return carry

    lax.fori_loop(0, TILES // QUARTER, backward_quarter, 0)
    pl.when(tp != LINE - 1)(g_out(1, TILES // QUARTER - 1).start)
    lax.fori_loop(0, TILES // QUARTER, forward_quarter, 0)

    def lead_in(tile, carry):
        for d in range(2):
            rate2, _, high, low, both = [
                jnp.broadcast_to(tabs[d, k, pl.ds(tile, 1), :], (SUBS, 128)) for k in range(5)
            ]
            g_re, g_im = stretch_decay(rate2, high, low, both, spans[0], spans[1])
            x_re, x_im = loc[tile, d, 0], loc[tile, d, 1]
            for hop in (1, 2, 4):
                turn = hop if d == 0 else SUBS - hop
                inside = sub8 >= hop if d == 0 else sub8 < SUBS - hop
                q_re, q_im, h_re, h_im = [pltpu.roll(v, turn, 0) for v in (x_re, x_im, g_re, g_im)]
                m_re, m_im = times(g_re, g_im, q_re, q_im)
                n_re, n_im = times(g_re, g_im, h_re, h_im)
                x_re, x_im = jnp.where(inside, x_re + m_re, x_re), jnp.where(inside, x_im + m_im, x_im)
                g_re, g_im = jnp.where(inside, n_re, g_re), jnp.where(inside, n_im, g_im)
            turn = 1 if d == 0 else SUBS - 1
            inside = sub8 >= 1 if d == 0 else sub8 < SUBS - 1
            x_re, x_im, g_re, g_im = [
                jnp.where(inside, pltpu.roll(v, turn, 0), blank_value)
                for v, blank_value in ((x_re, 0.0), (x_im, 0.0), (g_re, 1.0), (g_im, 0.0))
            ]
            lead[tile, d, 0] = x_re
            lead[tile, d, 1] = x_im
            fade[tile, d, 0] = g_re
            fade[tile, d, 1] = g_im
        return carry

    lane_group = lax.broadcasted_iota(jnp.int32, (64, 128), 1) // 16
    blank = jnp.zeros((64, 128), BF16)

    def spread(m, carry):
        for d in range(2):
            for part in range(2):
                sign = 1.0 if part == 0 else -1.0
                at = (d * 2 + part) * 128
                lower = (sout_v[d, part, pl.ds(m * 8, 8)].reshape(128, 64) * sign).T
                upper = (sout_v[d, part, pl.ds(TILES + m * 8, 8)].reshape(128, 64) * sign).T
                for i in range(8):
                    tile = m * 8 + i
                    cst[tile, at:at + 64, 0:128] = jnp.where(lane_group == i, lower, 0.0).astype(BF16)
                    cst[tile, at:at + 64, 128:256] = blank
                    cst[tile, at + 64:at + 128, 0:128] = blank
                    cst[tile, at + 64:at + 128, 128:256] = jnp.where(lane_group == i, upper, 0.0).astype(BF16)
        return carry


    def own_work():
        lax.fori_loop(0, TILES, lead_in, 0)
        lax.fori_loop(0, 4, spread, 0)

    def pass_on_elapsed():
        blocks(t_dev, LINE - 1, t_send.at[0], t_recv.at[0]).wait_recv()
        total = t_dev[0]
        for k in range(1, LINE):
            total = total + t_dev[k]
        t_line[sp] = total
        for k in range(1, LINES):
            peer, there = ahead(k)
            pl.when(there)(u_out(peer).start)

    c_sout.wait()

    @pl.when(core == 0)
    def _():
        own_work()

    pass_on_elapsed()

    g_in[tp] = ssum[way, yi]
    places = [jnp.where(way == 0, o, LINE - 1 - o) for o in range(LINE)]
    gains = [quarter_decay(t_dev[k]) for k in places]
    blocks(g_in, LINE - 1, g_send.at[0], g_recv.at[0]).wait_recv()
    zero, one = jnp.zeros((QUARTER, 128), F32), jnp.ones((QUARTER, 128), F32)
    run, run_d, before, before_d = (zero, zero), (one, zero), [], []
    for o, k in enumerate(places):
        before.append(run)
        before_d.append(run_d)
        moved = times(*gains[o], *run)
        run = (moved[0] + g_in[k, 0], moved[1] + g_in[k, 1])
        run_d = times(*gains[o], *run_d)
    x_in[sp, 0] = run[0]
    x_in[sp, 1] = run[1]
    for k in range(1, LINES):
        peer, there = ahead(k)
        pl.when(there)(x_out(peer).start)
    for o, k in enumerate(places):
        e_new[k, 0] = before[o][0]
        e_new[k, 1] = before[o][1]
        e_fade[k, 0] = before_d[o][0]
        e_fade[k, 1] = before_d[o][1]
    @pl.when(core == 1)
    def _():
        own_work()

    def local_pass(q, carry):
        total = resp[q]
        for t in range(QUARTER):
            tile = q * QUARTER + t
            for d in range(2):
                base = d * 256
                s_re, s_im = lead[tile, d, 0], lead[tile, d, 1]
                f_re, f_im = fade[tile, d, 0], fade[tile, d, 1]
                found = [None] * STEPS
                for j in range(STEPS) if d == 0 else range(STEPS - 1, -1, -1):
                    at = pl.ds(j * SUBS, SUBS)
                    a_re, a_im = dec[tile, at, base:base + 128], dec[tile, at, base + 128:base + 256]
                    n_re, n_im = times(a_re, a_im, s_re, s_im)
                    s_re = n_re + proj[tile, at, base:base + 128]
                    s_im = n_im + proj[tile, at, base + 128:base + 256]
                    f_re, f_im = times(a_re, a_im, f_re, f_im)
                    dec[tile, at, base:base + 128] = f_re
                    dec[tile, at, base + 128:base + 256] = f_im
                    found[j] = (s_re, s_im)
                    if j % 2 == (1 if d == 0 else 0):
                        first = j - j % 2
                        for part in range(2):
                            pair = jnp.concatenate([found[first][part], found[first + 1][part]], axis=0)
                            states[t, first * SUBS:(first + 2) * SUBS, base + part * 128:base + part * 128 + 128] = (
                                pair.astype(BF16)
                            )
            if t:
                total = total + jnp.dot(states[t - 1], cst[tile - 1], preferred_element_type=F32)
        resp[q] = total + jnp.dot(states[QUARTER - 1], cst[q * QUARTER + QUARTER - 1], preferred_element_type=F32)
        return carry

    lax.fori_loop(0, 2, local_pass, 0)

    blocks(t_dev, LINE - 1, t_send.at[0], t_recv.at[0]).wait_send()
    blocks(g_in, LINE - 1, g_send.at[0], g_recv.at[0]).wait_send()
    lines_out(t_line, u_send.at[0], u_recv.at[0])

    lines_in(t_line, u_send.at[0], u_recv.at[0])
    between = jnp.zeros((SUBS, 128), F32)
    for k in range(1, LINES):
        peer, there = behind(k)
        far_re, far_im = quarter_decay(between)
        x_far[k, 0] = far_re
        x_far[k, 1] = far_im
        between = between + jnp.where(there, t_line[peer], 0.0)

    lines_in(x_in, x_send.at[0], x_recv.at[0])
    gone = (zero, zero)
    for k in range(1, LINES):
        peer, there = behind(k)
        moved = times(x_far[k, 0], x_far[k, 1], x_in[peer, 0], x_in[peer, 1])
        gone = tuple(g + jnp.where(there, m, 0.0) for g, m in zip(gone, moved))
    for k in range(LINE):
        moved = times(e_fade[k, 0], e_fade[k, 1], *gone)
        e_new[k, 0] = e_new[k, 0] + moved[0]
        e_new[k, 1] = e_new[k, 1] + moved[1]
    for k in range(1, LINE):
        e_out(k).start()
    e_in[tp] = e_new[tp]
    def second_pass(d):
        base = d * 256
        for n in (3, 4):
            pl.when((core == d) == (n == 3))(blocks(e_in, n, e_send.at[0], e_recv.at[d]).wait_recv)

        def quarter(q, carry):
            total = resp[q]
            for t in range(QUARTER):
                tile = q * QUARTER + t
                e_re = jnp.broadcast_to(e_in[q * 2 + d, 0, t:t + 1, :], (16, 128))
                e_im = jnp.broadcast_to(e_in[q * 2 + d, 1, t:t + 1, :], (16, 128))
                for r in range(0, ROWS, 16):
                    f_re, f_im = dec[tile, r:r + 16, base:base + 128], dec[tile, r:r + 16, base + 128:base + 256]
                    m_re, m_im = times(f_re, f_im, e_re, e_im)
                    states[t, r:r + 16, base:base + 128] = m_re.astype(BF16)
                    states[t, r:r + 16, base + 128:base + 256] = m_im.astype(BF16)
                total = total + jnp.dot(
                    states[t, :, base:base + 256], cst[tile, base:base + 256, :], preferred_element_type=F32
                )
            resp[q] = total
            return carry

        for q in range(TILES // QUARTER):
            quarter(q, 0)

    lax.fori_loop(2, 4, local_pass, 0)
    lines_out(x_in, x_send.at[0], x_recv.at[0])
    second_pass(0)
    second_pass(1)

    c_glu.wait()
    c_ow.wait()

    blocks(e_in, LINE - 1, e_send.at[0], e_recv.at[0]).wait_send()


def output_unit(resp, glu_v, outw_v, gbias_v, ogain_v, out_ref):
    row_i = lax.broadcasted_iota(jnp.int32, (ROWS, ROWS), 0)
    col_i = lax.broadcasted_iota(jnp.int32, (ROWS, ROWS), 1)
    back = jnp.where(row_i == (col_i % SUBS) * STEPS + col_i // SUBS, 1.0, 0.0).astype(BF16)
    response = jnp.concatenate(
        [resp[m, :, 0:128] for m in range(4)] + [resp[m, :, 128:256] for m in range(4)], axis=1
    )
    active = jax.nn.gelu(response, approximate=True)
    active_low = active.astype(BF16)
    gates = []
    for n in range(4):
        at = slice(n * 256, (n + 1) * 256)
        gate = jnp.dot(active_low, glu_v[:, at], preferred_element_type=F32) + gbias_v[:, at]
        gates.append((active[:, at] * jax.nn.sigmoid(gate)).astype(BF16))
    gated = jnp.dot(back, jnp.concatenate(gates, axis=1), preferred_element_type=F32).astype(BF16)
    outs, square = [], None
    for n in range(8):
        at = slice(n * 256, (n + 1) * 256)
        piece = jnp.dot(gated, outw_v[:, at], preferred_element_type=F32)
        outs.append(piece)
        part = jnp.sum(piece * piece, axis=-1, keepdims=True)
        square = part if square is None else square + part
    scale = lax.rsqrt(square * (1.0 / 2048.0) + EPS)
    for n in range(8):
        at = slice(n * 256, (n + 1) * 256)
        out_ref[:, at] = (outs[n] * scale * ogain_v[:, at]).astype(BF16)


def local(
    tokens, elapsed, norm_gain, in_weight, state_input, state_output, forget_rate, decay_angle,
    skip_gain, glu_weight, glu_bias, out_weight, out_gain,
):
    args = (
        tokens, elapsed.reshape(1, -1), norm_gain.reshape(1, -1), in_weight, state_input.transpose(0, 1, 2, 4, 3),
        state_output, forget_rate, decay_angle, skip_gain.reshape(1, -1), glu_weight, out_weight,
    )
    vm = pltpu.VMEM
    scratch = [vm(a.shape, a.dtype) for a in args[:9]]
    scratch += [
        vm((ROWS, 2048), BF16),
        vm((ROWS, 1024), F32),
        vm((4, ROWS, 256), BF16),
        vm((4, 256, 512), BF16),
        vm((TILES, 512, 256), BF16),
        vm((TILES, ROWS, 512), F32),
        vm((TILES, ROWS, 512), F32),
        vm((2, 5, TILES, 128), F32),
        vm((2, ROWS, 128), BF16),
        vm((16, 128), F32),
        vm((QUARTER, 128, 256), BF16),
        vm((QUARTER // 2, 128, 256), BF16),
        vm((QUARTER // 2, ROWS, 256), F32),
        vm((QUARTER, ROWS, 512), BF16),
        vm((6, SUBS, 128), F32),
        vm((TILES, 2, 2, SUBS, 128), F32),
        vm((2, 4, 2, QUARTER, 128), F32),
        vm((TILES, 2, 2, SUBS, 128), F32),
        vm((TILES, 2, 2, SUBS, 128), F32),
        vm((LINE, SUBS, 128), F32),
        vm((LINES, SUBS, 128), F32),
        vm((LINE, 2, QUARTER, 128), F32),
        vm((LINES, 2, QUARTER, 128), F32),
        vm((LINES, 2, QUARTER, 128), F32),
        vm((LINE, 2, QUARTER, 128), F32),
        vm((LINE, 2, QUARTER, 128), F32),
        vm((LINE, 2, QUARTER, 128), F32),
        pltpu.SemaphoreType.DMA((15,)),
    ]
    scratch += [pltpu.SemaphoreType.DMA((n,)) for n in (1, 1, 1, 1, 1, 1, 1, 1, 1, 2)]
    inner = pl.BlockSpec(memory_space=pltpu.VMEM)
    response, glu_held, out_held = pl.pallas_call(
        kernel,
        out_shape=(
            vm((4, ROWS, 256), F32),
            vm(glu_weight.shape, BF16),
            vm(out_weight.shape, BF16),
        ),
        in_specs=[pl.BlockSpec(memory_space=pltpu.HBM)] * len(args),
        out_specs=(inner, inner, inner),
        scratch_shapes=scratch,
        compiler_params=pltpu.CompilerParams(
            collective_id=0, has_side_effects=True, vmem_limit_bytes=50000000
        ),
        name="ssm_layer",
    )(*args)
    return pl.pallas_call(
        output_unit,
        out_shape=jax.ShapeDtypeStruct(tokens.shape, BF16),
        in_specs=[inner] * 5,
        out_specs=inner,
        compiler_params=pltpu.CompilerParams(vmem_limit_bytes=16000000),
        name="output_unit",
    )(response, glu_held, out_held, glu_bias.reshape(1, -1), out_gain.reshape(1, -1))


def solution(mesh):
    rows = P(("sp", "tp"), None)
    placed = (rows, P(("sp", "tp")), P(), P(), P(), P(), P(), P(), P(), P(), P(), P(), P())
    return jax.shard_map(local, mesh=mesh, in_specs=placed, out_specs=rows, check_vma=False)
```

```python
import functools
import math

import jax
import jax.numpy as jnp
from jax import lax
from jax.experimental import pallas as pl
from jax.experimental.pallas import tpu as pltpu
from jax.sharding import PartitionSpec as P

F32 = jnp.float32
BF16 = jnp.bfloat16
MESH = pl.DeviceIdType.MESH

ROWS = 128
TILES = 32
SUBS = 8
STEPS = 16
LINE = 8
LINES = 16
QUARTER = 8
EPS = 1e-06
LOG2E = 1.4426950408889634
SIN_C = (4.442883014678955, -7.308241367340088, 3.6062889099121094, -0.845763623714447, 0.10920575261116028)
COS_C = (1.4142135381698608, -6.9788641929626465, 5.73988151550293, -1.8882750272750854, 0.3322518765926361, -0.034502167254686356)
POINTS = [1.5 + 1.5 * math.cos((2 * i + 1) * math.pi / 32.0) for i in range(16)]
WEIGHTS = [1.0 / math.prod(p - o for o in POINTS if o != p) for p in POINTS]
INV_TURN = 1.0 / (2.0 * math.pi)
TURN_HI = math.floor(INV_TURN * 4096.0) / 4096.0
TURN_LO = INV_TURN - TURN_HI


def horner(x, coefficients):
    total = coefficients[-1]
    for c in coefficients[-2::-1]:
        total = total * x + c
    return total


def half_turn_parts(turns):
    part = turns - lax.round(turns, lax.RoundingMethod.TO_NEAREST_EVEN)
    square = part * part
    return part * horner(square, SIN_C), horner(square, COS_C)


def decay_parts(size, turns):
    sine, cosine = half_turn_parts(turns)
    lean = size * sine
    return size - lean * sine, lean * cosine


def in_parts(value, count):
    parts = []
    for _ in range(count):
        parts.append(value.astype(BF16))
        value = value - parts[-1].astype(F32)
    return parts


def times(a_re, a_im, b_re, b_im):
    return a_re * b_re - a_im * b_im, a_re * b_im + a_im * b_re


def kernel(
    tokens_h, elapsed_h, ngain_h, inw_h, sin_h, sout_h, rate_h, angle_h, skip_h, glu_h, outw_h,
    resp, glu_v, outw_v,
    tokens_v, elapsed_v, ngain_v, inw_v, sin_v, sout_v, rate_v, angle_v, skip_v,
    normed, acc, drv, bst, cst, proj, dec, tabs, by_token, at_node, cell_decay, cell_gain, gain, states, spans, loc, ssum, lead, fade,
    t_dev, t_line, g_in, x_in, x_far, e_new, e_fade, e_in,
    dma_sem, t_send, t_recv, u_send, u_recv, g_send, g_recv, x_send, x_recv, e_send, e_recv,
):
    sp = lax.axis_index("sp")
    tp = lax.axis_index("tp")
    yi, core = tp // 2, tp % 2
    way = core

    def line_peer(k):
        return {"sp": sp, "tp": k}

    def plane_peer(k):
        return {"sp": k, "tp": tp}

    def remote(src, dst, send_sem, recv_sem, peer):
        return pltpu.make_async_remote_copy(
            src_ref=src, dst_ref=dst, send_sem=send_sem, recv_sem=recv_sem, device_id=peer, device_id_type=MESH,
        )

    def ahead(step):
        k = jnp.where(way == 0, sp + step, sp - step)
        return lax.rem(k + LINES, LINES), jnp.logical_and(k >= 0, k < LINES)

    def behind(step):
        return ahead(-step)

    pairs = [
        (elapsed_h, elapsed_v), (tokens_h, tokens_v), (ngain_h, ngain_v), (rate_h, rate_v), (angle_h, angle_v),
        (sin_h, sin_v), (sout_h, sout_v), (skip_h, skip_v), (glu_h, glu_v), (outw_h, outw_v),
    ]
    copies = [pltpu.make_async_copy(a, b, dma_sem.at[k]) for k, (a, b) in enumerate(pairs)]
    c_el, c_tok, c_ng, c_rate, c_ang, c_sin, c_sout, c_skip, c_glu, c_ow = copies
    in_copies = [
        pltpu.make_async_copy(inw_h.at[pl.ds(k * 512, 512), :], inw_v.at[pl.ds(k * 512, 512), :], dma_sem.at[11 + k])
        for k in range(4)
    ]
    for c in (c_el, c_tok, c_ng, c_rate, c_ang):
        c.start()
    for c in in_copies:
        c.start()
    for c in (c_sin, c_sout, c_skip, c_glu, c_ow):
        c.start()

    barrier = pltpu.get_barrier_semaphore()
    for k in range(1, LINE):
        pl.semaphore_signal(barrier, inc=1, device_id=line_peer(lax.rem(tp + k, LINE)), device_id_type=MESH)
    for k in range(1, LINES):
        pl.semaphore_signal(barrier, inc=1, device_id=plane_peer(lax.rem(sp + k, LINES)), device_id_type=MESH)

    c_el.wait()
    steps = elapsed_v[...]
    whole = jnp.floor(steps)
    rest = steps - whole
    lane8 = lax.broadcasted_iota(jnp.int32, (SUBS, 128), 1)
    sub8 = lax.broadcasted_iota(jnp.int32, (SUBS, 128), 0)

    def picked(mask, row):
        total = jnp.sum(jnp.where(mask, jnp.broadcast_to(row, (SUBS, 128)), 0.0), axis=1, keepdims=True)
        return jnp.broadcast_to(total, (SUBS, 128))

    t_dev[tp] = jnp.where(sub8 == 0, picked(lane8 >= 0, whole), picked(lane8 >= 0, rest))
    gaps = [steps - p for p in POINTS]
    upto, after = [jnp.ones_like(steps)], [jnp.ones_like(steps)]
    for k in range(15):
        upto.append(upto[-1] * gaps[k])
        after.append(after[-1] * gaps[15 - k])
    basis = [upto[k] * after[15 - k] * WEIGHTS[k] for k in range(16)]
    scale = basis[0]
    for b in basis[1:]:
        scale = scale + b
    basis = jnp.concatenate(basis, axis=0) / jnp.broadcast_to(scale, (16, 128))
    b1, b2, b3 = in_parts(basis, 3)
    r1, r2 = in_parts(basis * jnp.sqrt(steps), 2)
    none16 = jnp.zeros((16, 128), BF16)
    token_rows = jnp.concatenate([b1, b1, b2, b2, b1, b3, none16, none16], axis=0)
    gain_rows = jnp.concatenate([r1, r1, r2] + [none16] * 5, axis=0)
    row_i = lax.broadcasted_iota(jnp.int32, (ROWS, ROWS), 0)
    col_i = lax.broadcasted_iota(jnp.int32, (ROWS, ROWS), 1)
    order = jnp.where(col_i == (row_i % SUBS) * STEPS + row_i // SUBS, 1.0, 0.0).astype(BF16)
    across = (((1,), (1,)), ((), ()))
    for k, rows in enumerate((token_rows, gain_rows)):
        by_token[k] = lax.dot_general(order, rows, across, preferred_element_type=F32).astype(BF16)
    node_i = lax.broadcasted_iota(jnp.int32, (16, 128), 0)
    nodes = jnp.full((16, 128), POINTS[0], F32)
    for k in range(1, 16):
        nodes = jnp.where(node_i == k, POINTS[k], nodes)
    at_node[...] = nodes
    none32 = jnp.zeros((32, 256), BF16)
    none80 = jnp.zeros((80, 256), BF16)
    for t in range(QUARTER):
        cell_decay[t, 96:128, :] = none32
    for t in range(QUARTER // 2):
        cell_gain[t, 48:128, :] = none80
    stretch = lane8 // STEPS
    for k, mask in enumerate((stretch == sub8, stretch > sub8, stretch < sub8)):
        spans[2 * k] = picked(mask, whole)
        spans[2 * k + 1] = picked(mask, rest)

    def t_out(k):
        return remote(t_dev.at[tp], t_dev.at[tp], t_send.at[0], t_recv.at[0], line_peer(lax.rem(tp + k, LINE)))

    def u_out(peer):
        return remote(t_line.at[sp], t_line.at[sp], u_send.at[0], u_recv.at[0], plane_peer(peer))

    def x_out(peer):
        return remote(x_in.at[sp], x_in.at[sp], x_send.at[0], x_recv.at[0], plane_peer(peer))

    def g_out(d, q):
        return remote(ssum.at[d, q], g_in.at[tp], g_send.at[0], g_recv.at[0], line_peer(q * 2 + d))

    def e_out(k):
        peer = lax.rem(tp + k, LINE)
        return remote(e_new.at[peer], e_in.at[tp], e_send.at[0], e_recv.at[core], line_peer(peer))

    def blocks(buf, n, send_sem, recv_sem):
        part = buf.at[pl.ds(0, n)]
        return remote(part, part, send_sem, recv_sem, line_peer(lax.rem(tp + 1, LINE)))

    lines_behind = jnp.where(way == 0, sp, LINES - 1 - sp)
    lines_ahead = LINES - 1 - lines_behind

    def lines_in(buf, send_sem, recv_sem):
        for n in range(1, LINES):
            pl.when(lines_behind == n)(blocks(buf, n, send_sem, recv_sem).wait_recv)

    def lines_out(buf, send_sem, recv_sem):
        for n in range(1, LINES):
            pl.when(lines_ahead == n)(blocks(buf, n, send_sem, recv_sem).wait_send)

    c_rate.wait()
    c_ang.wait()
    for d in range(2):
        rate = jnp.concatenate([rate_v[d, 0:TILES, :], rate_v[d, TILES:, :]], axis=1)
        angle = jnp.concatenate([angle_v[d, 0:TILES, :], angle_v[d, TILES:, :]], axis=1)
        tabs[d, 0] = rate * (-LOG2E)
        tabs[d, 1] = rate * 2.0
        big = lax.round(angle * 1024.0, lax.RoundingMethod.TO_NEAREST_EVEN) * (1.0 / 1024.0)
        small = angle - big
        first = big * TURN_HI
        second = big * TURN_LO + (small * TURN_HI + small * TURN_LO)
        high = lax.round(first * 256.0, lax.RoundingMethod.TO_NEAREST_EVEN) * (1.0 / 256.0)
        low = (first - high) + second
        tabs[d, 2] = high
        tabs[d, 3] = low
        tabs[d, 4] = high + low

    def stretch_decay(rate2, high, low, both, t_whole, t_rest):
        size = jnp.exp2(rate2 * (t_whole + t_rest))
        turns = high * t_whole
        turns = turns - lax.round(turns, lax.RoundingMethod.TO_NEAREST_EVEN)
        return decay_parts(size, turns + low * t_whole + both * t_rest)

    def quarter_decay(t_tile):
        t_whole = jnp.broadcast_to(t_tile[0:1, :], (QUARTER, 128))
        t_rest = jnp.broadcast_to(t_tile[1:2, :], (QUARTER, 128))
        rows = pl.ds(pl.multiple_of(yi * QUARTER, QUARTER), QUARTER)
        return stretch_decay(*[tabs[way, k, rows, :] for k in (0, 2, 3, 4)], t_whole, t_rest)

    c_tok.wait()
    c_ng.wait()
    for r in range(4):
        x = tokens_v[pl.ds(r * 32, 32), :].astype(F32)
        scale = lax.rsqrt(jnp.mean(x * x, axis=-1, keepdims=True) + EPS)
        normed[pl.ds(r * 32, 32), :] = (x * scale * ngain_v[...]).astype(BF16)

    for k in range(4):
        in_copies[k].wait()
        part = jnp.dot(normed[:, k * 512:(k + 1) * 512], inw_v[k * 512:(k + 1) * 512, :], preferred_element_type=F32)
        acc[...] = part if k == 0 else acc[...] + part

    driven = jnp.dot(order, acc[...].astype(BF16), preferred_element_type=F32)
    c_skip.wait()
    for m in range(4):
        low_d, high_d = driven[:, m * 128:(m + 1) * 128], driven[:, 512 + m * 128:512 + (m + 1) * 128]
        resp[m, :, 0:128] = low_d * skip_v[:, m * 128:(m + 1) * 128]
        resp[m, :, 128:256] = high_d * skip_v[:, 512 + m * 128:512 + (m + 1) * 128]
        drv[m, :, 0:128] = low_d.astype(BF16)
        drv[m, :, 128:256] = high_d.astype(BF16)

    c_sin.wait()
    nothing = jnp.zeros((128, 64), BF16)
    for m in range(4):
        for d in range(2):
            for part in range(2):
                at = (d * 2 + part) * 128
                lower = sin_v[d, part, m * 8:(m + 1) * 8].reshape(128, 64)
                upper = sin_v[d, part, TILES + m * 8:TILES + (m + 1) * 8].reshape(128, 64)
                bst[m, 0:128, at:at + 128] = jnp.concatenate([lower, nothing], axis=1)
                bst[m, 128:256, at:at + 128] = jnp.concatenate([nothing, upper], axis=1)

    group_lane = (lax.broadcasted_iota(jnp.int32, (ROWS, 256), 1) // 16) % 8

    def first_pass(d, q):
        base = d * 256

        def values_at_nodes(t):
            row = pl.ds(q * QUARTER + t, 1)
            x = at_node[...]
            rate2, double, both = [jnp.broadcast_to(tabs[d, k, row, :], (16, 128)) for k in (0, 1, 4)]
            size = jnp.exp2(rate2 * x)
            y = double * x
            near = y * horner(y, (1.0, -0.5, 1.0 / 6.0, -1.0 / 24.0))
            gap = jnp.where(y < 0.03, near, 1.0 - size * size)
            for part, value in enumerate(decay_parts(size, both * x)):
                v1, v2, v3 = in_parts(value, 3)
                for k, v in enumerate((v1, v2, v1, v2, v3, v1)):
                    cell_decay[t, k * 16:(k + 1) * 16, part * 128:(part + 1) * 128] = v
            g1, g2 = in_parts(gap * lax.rsqrt(jnp.maximum(gap * x, 1e-37)), 2)
            at = slice(t % 2 * 128, t % 2 * 128 + 128)
            for k, v in enumerate((g1, g2, g1)):
                cell_gain[t // 2, k * 16:(k + 1) * 16, at] = v

        def products(t):
            gain[t // 2] = jnp.dot(by_token[1], cell_gain[t // 2], preferred_element_type=F32)
            for u in (t, t + 1):
                tile = q * QUARTER + u
                dec[tile, :, base:base + 256] = jnp.dot(by_token[0], cell_decay[u], preferred_element_type=F32)
                lhs = drv[q] * jnp.where(group_lane == u, 1.0, 0.0).astype(BF16)
                proj[tile, :, base:base + 256] = jnp.dot(
                    lhs, bst[q, :, base:base + 256], preferred_element_type=F32
                )

        def scan(t):
            tile = q * QUARTER + t
            s_re = s_im = None
            for j in range(STEPS) if d == 0 else range(STEPS - 1, -1, -1):
                at = pl.ds(j * SUBS, SUBS)
                damp = gain[t // 2, at, t % 2 * 128:t % 2 * 128 + 128]
                p_re = proj[tile, at, base:base + 128] * damp
                p_im = proj[tile, at, base + 128:base + 256] * damp
                proj[tile, at, base:base + 128] = p_re
                proj[tile, at, base + 128:base + 256] = p_im
                if s_re is None:
                    s_re, s_im = p_re, p_im
                else:
                    a_re, a_im = dec[tile, at, base:base + 128], dec[tile, at, base + 128:base + 256]
                    n_re, n_im = times(a_re, a_im, s_re, s_im)
                    s_re, s_im = n_re + p_re, n_im + p_im
            loc[tile, d, 0] = s_re
            loc[tile, d, 1] = s_im
            k = 2 if d == 0 else 4
            rate2, high, low, both = [
                jnp.broadcast_to(tabs[d, i, pl.ds(tile, 1), :], (SUBS, 128)) for i in (0, 2, 3, 4)
            ]
            w_re, w_im = stretch_decay(rate2, high, low, both, spans[k], spans[k + 1])
            m_re, m_im = times(w_re, w_im, s_re, s_im)
            ssum[d, q, 0, t:t + 1, :] = jnp.sum(m_re, axis=0, keepdims=True)
            ssum[d, q, 1, t:t + 1, :] = jnp.sum(m_im, axis=0, keepdims=True)

        for t in (0, 1):
            values_at_nodes(t)
        products(0)
        for t in (2, 3):
            values_at_nodes(t)
        for t in range(0, QUARTER, 2):
            if t + 2 < QUARTER:
                products(t + 2)
            for u in (t, t + 1):
                if u + 4 < QUARTER:
                    values_at_nodes(u + 4)
                scan(u)

    def backward_quarter(q, carry):
        @pl.when(q == 2)
        def _():
            pl.semaphore_wait(barrier, LINE - 1 + LINES - 1)
            for k in range(1, LINE):
                t_out(k).start()
            pl.when(tp != 1)(g_out(1, 0).start)

        pl.when(jnp.logical_and(q >= 2, tp != q * 2 - 1))(g_out(1, q - 1).start)

        first_pass(1, q)
        return carry

    def forward_quarter(q, carry):
        first_pass(0, q)
        pl.when(tp != q * 2)(g_out(0, q).start)
        return carry

    lax.fori_loop(0, TILES // QUARTER, backward_quarter, 0)
    pl.when(tp != LINE - 1)(g_out(1, TILES // QUARTER - 1).start)
    lax.fori_loop(0, TILES // QUARTER, forward_quarter, 0)

    def lead_in(tile, carry):
        for d in range(2):
            rate2, _, high, low, both = [
                jnp.broadcast_to(tabs[d, k, pl.ds(tile, 1), :], (SUBS, 128)) for k in range(5)
            ]
            g_re, g_im = stretch_decay(rate2, high, low, both, spans[0], spans[1])
            x_re, x_im = loc[tile, d, 0], loc[tile, d, 1]
            for hop in (1, 2, 4):
                turn = hop if d == 0 else SUBS - hop
                inside = sub8 >= hop if d == 0 else sub8 < SUBS - hop
                q_re, q_im, h_re, h_im = [pltpu.roll(v, turn, 0) for v in (x_re, x_im, g_re, g_im)]
                m_re, m_im = times(g_re, g_im, q_re, q_im)
                n_re, n_im = times(g_re, g_im, h_re, h_im)
                x_re, x_im = jnp.where(inside, x_re + m_re, x_re), jnp.where(inside, x_im + m_im, x_im)
                g_re, g_im = jnp.where(inside, n_re, g_re), jnp.where(inside, n_im, g_im)
            turn = 1 if d == 0 else SUBS - 1
            inside = sub8 >= 1 if d == 0 else sub8 < SUBS - 1
            x_re, x_im, g_re, g_im = [
                jnp.where(inside, pltpu.roll(v, turn, 0), blank_value)
                for v, blank_value in ((x_re, 0.0), (x_im, 0.0), (g_re, 1.0), (g_im, 0.0))
            ]
            lead[tile, d, 0] = x_re
            lead[tile, d, 1] = x_im
            fade[tile, d, 0] = g_re
            fade[tile, d, 1] = g_im
        return carry

    lane_group = lax.broadcasted_iota(jnp.int32, (64, 128), 1) // 16
    blank = jnp.zeros((64, 128), BF16)

    def spread(m, carry):
        for d in range(2):
            for part in range(2):
                sign = 1.0 if part == 0 else -1.0
                at = (d * 2 + part) * 128
                lower = (sout_v[d, part, pl.ds(m * 8, 8)].reshape(128, 64) * sign).T
                upper = (sout_v[d, part, pl.ds(TILES + m * 8, 8)].reshape(128, 64) * sign).T
                for i in range(8):
                    tile = m * 8 + i
                    cst[tile, at:at + 64, 0:128] = jnp.where(lane_group == i, lower, 0.0).astype(BF16)
                    cst[tile, at:at + 64, 128:256] = blank
                    cst[tile, at + 64:at + 128, 0:128] = blank
                    cst[tile, at + 64:at + 128, 128:256] = jnp.where(lane_group == i, upper, 0.0).astype(BF16)
        return carry


    def own_work():
        def four(r, carry):
            for t in range(4):
                lead_in(r * 4 + t, carry)
            return carry

        lax.fori_loop(0, TILES // 4, four, 0)
        lax.fori_loop(0, 4, spread, 0)

    def pass_on_elapsed():
        blocks(t_dev, LINE - 1, t_send.at[0], t_recv.at[0]).wait_recv()
        total = t_dev[0]
        for k in range(1, LINE):
            total = total + t_dev[k]
        t_line[sp] = total
        for k in range(1, LINES):
            peer, there = ahead(k)
            pl.when(there)(u_out(peer).start)

    c_sout.wait()

    @pl.when(core == 0)
    def _():
        own_work()

    pass_on_elapsed()

    g_in[tp] = ssum[way, yi]
    places = [jnp.where(way == 0, o, LINE - 1 - o) for o in range(LINE)]
    gains = [quarter_decay(t_dev[k]) for k in places]
    blocks(g_in, LINE - 1, g_send.at[0], g_recv.at[0]).wait_recv()
    zero, one = jnp.zeros((QUARTER, 128), F32), jnp.ones((QUARTER, 128), F32)
    run, run_d, before, before_d = (zero, zero), (one, zero), [], []
    for o, k in enumerate(places):
        before.append(run)
        before_d.append(run_d)
        moved = times(*gains[o], *run)
        run = (moved[0] + g_in[k, 0], moved[1] + g_in[k, 1])
        run_d = times(*gains[o], *run_d)
    x_in[sp, 0] = run[0]
    x_in[sp, 1] = run[1]
    for k in range(1, LINES):
        peer, there = ahead(k)
        pl.when(there)(x_out(peer).start)
    for o, k in enumerate(places):
        e_new[k, 0] = before[o][0]
        e_new[k, 1] = before[o][1]
        e_fade[k, 0] = before_d[o][0]
        e_fade[k, 1] = before_d[o][1]
    @pl.when(core == 1)
    def _():
        own_work()

    def local_pass(q, carry):
        total = resp[q]
        for t in range(QUARTER):
            tile = q * QUARTER + t
            for d in range(2):
                base = d * 256
                s_re, s_im = lead[tile, d, 0], lead[tile, d, 1]
                f_re, f_im = fade[tile, d, 0], fade[tile, d, 1]
                found = [None] * STEPS
                for j in range(STEPS) if d == 0 else range(STEPS - 1, -1, -1):
                    at = pl.ds(j * SUBS, SUBS)
                    a_re, a_im = dec[tile, at, base:base + 128], dec[tile, at, base + 128:base + 256]
                    n_re, n_im = times(a_re, a_im, s_re, s_im)
                    s_re = n_re + proj[tile, at, base:base + 128]
                    s_im = n_im + proj[tile, at, base + 128:base + 256]
                    f_re, f_im = times(a_re, a_im, f_re, f_im)
                    dec[tile, at, base:base + 128] = f_re
                    dec[tile, at, base + 128:base + 256] = f_im
                    found[j] = (s_re, s_im)
                    if j % 2 == (1 if d == 0 else 0):
                        first = j - j % 2
                        for part in range(2):
                            pair = jnp.concatenate([found[first][part], found[first + 1][part]], axis=0)
                            states[t, first * SUBS:(first + 2) * SUBS, base + part * 128:base + part * 128 + 128] = (
                                pair.astype(BF16)
                            )
            if t:
                total = total + jnp.dot(states[t - 1], cst[tile - 1], preferred_element_type=F32)
        resp[q] = total + jnp.dot(states[QUARTER - 1], cst[q * QUARTER + QUARTER - 1], preferred_element_type=F32)
        return carry

    lax.fori_loop(0, 2, local_pass, 0)

    blocks(t_dev, LINE - 1, t_send.at[0], t_recv.at[0]).wait_send()
    blocks(g_in, LINE - 1, g_send.at[0], g_recv.at[0]).wait_send()
    lines_out(t_line, u_send.at[0], u_recv.at[0])

    lines_in(t_line, u_send.at[0], u_recv.at[0])
    between = jnp.zeros((SUBS, 128), F32)
    for k in range(1, LINES):
        peer, there = behind(k)
        far_re, far_im = quarter_decay(between)
        x_far[k, 0] = far_re
        x_far[k, 1] = far_im
        between = between + jnp.where(there, t_line[peer], 0.0)

    lines_in(x_in, x_send.at[0], x_recv.at[0])
    gone = (zero, zero)
    for k in range(1, LINES):
        peer, there = behind(k)
        moved = times(x_far[k, 0], x_far[k, 1], x_in[peer, 0], x_in[peer, 1])
        gone = tuple(g + jnp.where(there, m, 0.0) for g, m in zip(gone, moved))
    for k in range(LINE):
        moved = times(e_fade[k, 0], e_fade[k, 1], *gone)
        e_new[k, 0] = e_new[k, 0] + moved[0]
        e_new[k, 1] = e_new[k, 1] + moved[1]
    for k in range(1, LINE):
        e_out(k).start()
    e_in[tp] = e_new[tp]
    def second_pass(d):
        base = d * 256
        for n in (3, 4):
            pl.when((core == d) == (n == 3))(blocks(e_in, n, e_send.at[0], e_recv.at[d]).wait_recv)

        def quarter(q, carry):
            total = resp[q]
            for t in range(QUARTER):
                tile = q * QUARTER + t
                e_re = jnp.broadcast_to(e_in[q * 2 + d, 0, t:t + 1, :], (16, 128))
                e_im = jnp.broadcast_to(e_in[q * 2 + d, 1, t:t + 1, :], (16, 128))
                for r in range(0, ROWS, 16):
                    f_re, f_im = dec[tile, r:r + 16, base:base + 128], dec[tile, r:r + 16, base + 128:base + 256]
                    m_re, m_im = times(f_re, f_im, e_re, e_im)
                    states[t, r:r + 16, base:base + 128] = m_re.astype(BF16)
                    states[t, r:r + 16, base + 128:base + 256] = m_im.astype(BF16)
                total = total + jnp.dot(
                    states[t, :, base:base + 256], cst[tile, base:base + 256, :], preferred_element_type=F32
                )
            resp[q] = total
            return carry

        for q in range(TILES // QUARTER):
            quarter(q, 0)

    lax.fori_loop(2, 4, local_pass, 0)
    lines_out(x_in, x_send.at[0], x_recv.at[0])
    second_pass(0)
    second_pass(1)

    c_glu.wait()
    c_ow.wait()

    blocks(e_in, LINE - 1, e_send.at[0], e_recv.at[0]).wait_send()


def output_unit(resp, glu_v, outw_v, gbias_v, ogain_v, out_ref, held, sems):
    row_i = lax.broadcasted_iota(jnp.int32, (ROWS, ROWS), 0)
    col_i = lax.broadcasted_iota(jnp.int32, (ROWS, ROWS), 1)
    back = jnp.where(row_i == (col_i % SUBS) * STEPS + col_i // SUBS, 1.0, 0.0).astype(BF16)
    response = jnp.concatenate(
        [resp[m, :, 0:128] for m in range(4)] + [resp[m, :, 128:256] for m in range(4)], axis=1
    )
    active = jax.nn.gelu(response, approximate=True)
    active_low = active.astype(BF16)
    gates = []
    for n in range(4):
        at = slice(n * 256, (n + 1) * 256)
        gate = jnp.dot(active_low, glu_v[:, at], preferred_element_type=F32) + gbias_v[:, at]
        gates.append((active[:, at] * jax.nn.sigmoid(gate)).astype(BF16))
    gated = jnp.dot(back, jnp.concatenate(gates, axis=1), preferred_element_type=F32).astype(BF16)
    outs, square = [], None
    for n in range(8):
        at = slice(n * 256, (n + 1) * 256)
        piece = jnp.dot(gated, outw_v[:, at], preferred_element_type=F32)
        outs.append(piece)
        part = jnp.sum(piece * piece, axis=-1, keepdims=True)
        square = part if square is None else square + part
    scale = lax.rsqrt(square * (1.0 / 2048.0) + EPS)
    sent = []
    for r in range(0, ROWS, 32):
        for n in range(8):
            at = slice(n * 256, (n + 1) * 256)
            held[r:r + 32, at] = (outs[n][r:r + 32] * scale[r:r + 32] * ogain_v[:, at]).astype(BF16)
        rows = pl.ds(r, 32)
        sent.append(pltpu.make_async_copy(held.at[rows, :], out_ref.at[rows, :], sems.at[r // 32]))
        sent[-1].start()
    for c in sent:
        c.wait()


def local(
    tokens, elapsed, norm_gain, in_weight, state_input, state_output, forget_rate, decay_angle,
    skip_gain, glu_weight, glu_bias, out_weight, out_gain,
):
    args = (
        tokens, elapsed.reshape(1, -1), norm_gain.reshape(1, -1), in_weight, state_input.transpose(0, 1, 2, 4, 3),
        state_output, forget_rate, decay_angle, skip_gain.reshape(1, -1), glu_weight, out_weight,
    )
    vm = pltpu.VMEM
    scratch = [vm(a.shape, a.dtype) for a in args[:9]]
    scratch += [
        vm((ROWS, 2048), BF16),
        vm((ROWS, 1024), F32),
        vm((4, ROWS, 256), BF16),
        vm((4, 256, 512), BF16),
        vm((TILES, 512, 256), BF16),
        vm((TILES, ROWS, 512), F32),
        vm((TILES, ROWS, 512), F32),
        vm((2, 5, TILES, 128), F32),
        vm((2, ROWS, 128), BF16),
        vm((16, 128), F32),
        vm((QUARTER, 128, 256), BF16),
        vm((QUARTER // 2, 128, 256), BF16),
        vm((QUARTER // 2, ROWS, 256), F32),
        vm((QUARTER, ROWS, 512), BF16),
        vm((6, SUBS, 128), F32),
        vm((TILES, 2, 2, SUBS, 128), F32),
        vm((2, 4, 2, QUARTER, 128), F32),
        vm((TILES, 2, 2, SUBS, 128), F32),
        vm((TILES, 2, 2, SUBS, 128), F32),
        vm((LINE, SUBS, 128), F32),
        vm((LINES, SUBS, 128), F32),
        vm((LINE, 2, QUARTER, 128), F32),
        vm((LINES, 2, QUARTER, 128), F32),
        vm((LINES, 2, QUARTER, 128), F32),
        vm((LINE, 2, QUARTER, 128), F32),
        vm((LINE, 2, QUARTER, 128), F32),
        vm((LINE, 2, QUARTER, 128), F32),
        pltpu.SemaphoreType.DMA((15,)),
    ]
    scratch += [pltpu.SemaphoreType.DMA((n,)) for n in (1, 1, 1, 1, 1, 1, 1, 1, 1, 2)]
    inner = pl.BlockSpec(memory_space=pltpu.VMEM)
    response, glu_held, out_held = pl.pallas_call(
        kernel,
        out_shape=(
            vm((4, ROWS, 256), F32),
            vm(glu_weight.shape, BF16),
            vm(out_weight.shape, BF16),
        ),
        in_specs=[pl.BlockSpec(memory_space=pltpu.HBM)] * len(args),
        out_specs=(inner, inner, inner),
        scratch_shapes=scratch,
        compiler_params=pltpu.CompilerParams(
            collective_id=0, has_side_effects=True, vmem_limit_bytes=50000000
        ),
        name="ssm_layer",
    )(*args)
    return pl.pallas_call(
        output_unit,
        out_shape=jax.ShapeDtypeStruct(tokens.shape, BF16),
        in_specs=[inner] * 5,
        out_specs=pl.BlockSpec(memory_space=pltpu.HBM),
        scratch_shapes=[vm(tokens.shape, BF16), pltpu.SemaphoreType.DMA((4,))],
        compiler_params=pltpu.CompilerParams(vmem_limit_bytes=16000000),
        name="output_unit",
    )(response, glu_held, out_held, glu_bias.reshape(1, -1), out_gain.reshape(1, -1))


def solution(mesh):
    rows = P(("sp", "tp"), None)
    placed = (rows, P(("sp", "tp")), P(), P(), P(), P(), P(), P(), P(), P(), P(), P(), P())
    return jax.shard_map(local, mesh=mesh, in_specs=placed, out_specs=rows, check_vma=False)
```
